32 devices in a mesh: sp: 8 (over z, y), tp: 4 (over x, core).
Axes of the slice: x: 2, y: 2, z: 4, core: 2. Of those that a mesh axis runs over, the one named last changes fastest.
Arguments:
- resid: bfloat16 [8192, 2048], P(('sp', 'tp')), may hold values from -6 to 6
- queries: bfloat16 [8192, 2048], P('sp', 'tp'), may hold values from -6 to 6
- keys: bfloat16 [8192, 2048], P('sp', 'tp'), may hold values from -6 to 6
- values: bfloat16 [8192, 4096], P('sp', 'tp'), may hold values from -6 to 6
- gates: bfloat16 [8192, 4096], P('sp', 'tp'), may hold values from -6 to 6
- log_decay: float32 [8, 8192], P('tp', 'sp'), may hold values from -1 to 0
- retention_output_weight: bfloat16 [4096, 2048], P('tp'), may hold values from -0.125 to 0.125
- norm_gain: bfloat16 [2048], replicated, may hold values from 0.099609375 to 1.8984375
- up_weight: bfloat16 [2048, 8192], P('sp', 'tp'), may hold values from -0.125 to 0.125
- down_weight: bfloat16 [8192, 2048], P('tp', 'sp'), may hold values from -0.0625 to 0.0625
Outputs:
- layer_out: bfloat16 [8192, 2048], P(('sp', 'tp'))
The draws below stay inside these ranges and needn't reach their ends.
All inputs are finite; a program needn't handle non-finite values.
Results may differ from the reference program's by a relative error of at most 0.02.
Values may be sent and summed in bfloat16 or wider, within the bound.
A program may use at most 128 MiB of HBM per device.

```python
import math
import jax
import jax.numpy as jnp
from jax import lax

D = 2048
HEADS = 8
DK = 256
DV = 512
FF = 8192
BLOCK = 128
TOK_DEV = 1024
SEQ = 8192
N_TP = 4


def draw_log_decay(key, part):
    key_sequence_order, key_reach, key_block, key_jitter, key_place, key_keep = jax.random.split(jax.random.fold_in(key, 7), 6)
    order = jax.random.permutation(key_sequence_order, HEADS)
    fast = order < HEADS // 2
    reach = jnp.exp(jax.random.uniform(key_reach, (HEADS,), jnp.float32, math.log(30.0), math.log(100.0)))
    fast_rate = -math.log(10.0) / reach
    slow_rate = jnp.full((HEADS,), -0.1 * math.log(10.0) / SEQ, jnp.float32)
    rate = jnp.where(fast, fast_rate, slow_rate)
    segments = SEQ // TOK_DEV
    factor = jnp.exp(jax.random.uniform(key_block, (HEADS, segments, 1), jnp.float32, math.log(0.5), math.log(2.0)))
    jitter = jnp.exp(jax.random.uniform(key_jitter, (HEADS, segments, TOK_DEV), jnp.float32, -0.5, 0.5))
    per_token_slot = (rate[:, None, None] * factor * jitter).reshape(HEADS, SEQ)
    places = jax.random.randint(key_place, (HEADS, 2), 0, SEQ)
    surviving_items = jax.random.uniform(key_keep, (HEADS, 2), jnp.float32, 0.5, 0.8)
    agreement_count = jnp.arange(SEQ)[None, None, :] == places[:, :, None]
    cluster_bundles = jnp.sum(jnp.where(agreement_count, jnp.log(surviving_items)[:, :, None], 0.0), axis=1)
    return (per_token_slot + cluster_bundles).astype(jnp.float32)


def block_scale(key, dims, cuts, smallest, top_value):
    loudness, own = 1.0, jax.random.fold_in(key, 6)
    for dim, blocks in cuts:
        draws = jnp.exp(jax.random.uniform(jax.random.fold_in(own, dim), (blocks,), jnp.float32, smallest / len(cuts), top_value / len(cuts)))
        loudness = loudness * jnp.repeat(draws, dims[dim] // blocks).reshape([-1 if axis == dim else 1 for axis in range(len(dims))])
    return loudness


def normal_values(rng, dims, scale, limit, pieces=(), held_as=jnp.bfloat16):
    array = scale * jax.random.normal(rng, dims, jnp.float32)
    if pieces:
        array = array * block_scale(rng, dims, pieces, -0.22, 0.18)
    return jnp.clip(array, -limit, limit).astype(held_as)


def setup_inputs(seed: int = 0) -> dict:
    arg_keys = jax.random.split(jax.random.key(seed), 11)
    return {
        "resid": normal_values(arg_keys[0], (SEQ, D), 1.0, 6.0, ((0, 32),)),
        "queries": normal_values(arg_keys[1], (SEQ, HEADS * DK), 1.0, 6.0, ((0, 8), (1, 4))),
        "keys": normal_values(arg_keys[2], (SEQ, HEADS * DK), 1.0, 6.0, ((0, 8), (1, 4))),
        "values": normal_values(arg_keys[3], (SEQ, HEADS * DV), 1.0, 6.0, ((0, 8), (1, 4))),
        "gates": normal_values(arg_keys[4], (SEQ, HEADS * DV), 1.0, 6.0, ((0, 8), (1, 4))),
        "log_decay": draw_log_decay(jax.random.fold_in(arg_keys[10], 71), 0),
        "retention_output_weight": normal_values(arg_keys[6], (HEADS * DV, D), (HEADS * DV // 2) ** -0.5, 0.125, ((0, 4),)),
        "norm_gain": jnp.clip(1.0 + 0.18 * jax.random.normal(arg_keys[7], (D,), jnp.float32), 0.099609375, 1.8984375).astype(jnp.bfloat16),
        "up_weight": normal_values(arg_keys[8], (D, FF), D ** -0.5, 0.125, ((0, 8), (1, 4))),
        "down_weight": normal_values(arg_keys[9], (FF, D), FF ** -0.5, 0.0625, ((0, 4), (1, 8))),
    }


tiny_stabilizer = 1e-06

def round_trip(values_in):
    return lax.optimization_barrier(values_in.astype(jnp.bfloat16)).astype(jnp.float32)

def rotate(values_in, token_indices):
    half_width = values_in.shape[-1] // 2
    inverse = 10000.0 ** (-jnp.arange(0, 2 * half_width, 2, dtype=jnp.float32) / (2 * half_width))
    angles = token_indices[:, None].astype(jnp.float32) * inverse[None, :]
    cosine = jnp.cos(angles)[:, None, :]
    sine_lookup = jnp.sin(angles)[:, None, :]
    first_half = values_in[..., :half_width]
    second = values_in[..., half_width:]
    return jnp.concatenate([first_half * cosine - second * sine_lookup, first_half * sine_lookup + second * cosine], axis=-1)

def normalize(updated, norm_gain):
    widened = updated.astype(jnp.float32)
    scaled = widened * lax.rsqrt(lax.optimization_barrier(jnp.mean(widened * widened, axis=-1, keepdims=True)) + tiny_stabilizer)
    return (scaled * norm_gain.astype(jnp.float32)).astype(jnp.bfloat16)

def block_step(carry_state, per_block):
    query_blk, key_blk, value_blk, gate_blk, cum_blk = per_block
    length = cum_blk.shape[1]
    causal = jnp.arange(length)[:, None] >= jnp.arange(length)[None, :]
    spread = cum_blk[:, :, None] - cum_blk[:, None, :]
    factor = jnp.where(causal[None], jnp.exp(jnp.minimum(spread, 0.0)), 0.0)
    scores = jnp.einsum('ihd,jhd->hij', query_blk, key_blk)
    weights = round_trip(scores * factor)
    within_block = jnp.einsum('hij,jhv->ihv', weights, value_blk)
    decayed = round_trip(query_blk * jnp.exp(cum_blk).T[:, :, None])
    carried_part = jnp.einsum('ihd,hdv->ihv', decayed, round_trip(carry_state))
    retained = within_block + carried_part
    normed = retained * lax.rsqrt(lax.optimization_barrier(jnp.mean(retained * retained, axis=-1, keepdims=True)) + tiny_stabilizer)
    gated_out = (jax.nn.silu(gate_blk) * normed).astype(jnp.bfloat16)
    tile_count_all = cum_blk[:, -1]
    key_decayed = round_trip(key_blk * jnp.exp(tile_count_all[:, None] - cum_blk).T[:, :, None])
    update = jnp.einsum('jhd,jhv->hdv', key_decayed, value_blk)
    return (jnp.exp(tile_count_all)[:, None, None] * carry_state + update, gated_out)

def grouped_product(left, right, groups):
    group_width = left.shape[1] // groups

    def add_group(running, number):
        first_row = (number * group_width).astype(jnp.int32)
        left_part = lax.dynamic_slice_in_dim(left, first_row, group_width, 1)
        right_part = lax.dynamic_slice_in_dim(right, first_row, group_width, 0)
        partial_value = jnp.dot(left_part, right_part, preferred_element_type=jnp.float32)
        return (running + round_trip(partial_value), None)
    running = jnp.zeros((left.shape[0], right.shape[1]), jnp.float32)
    running, unused = lax.scan(add_group, running, jnp.arange(groups, dtype=jnp.int32))
    return running

def channel_mixer(normed, up_weight, down_weight, groups):
    group_width = up_weight.shape[1] // groups

    def add_group(running, number):
        first_row = (number * group_width).astype(jnp.int32)
        up_part = lax.dynamic_slice_in_dim(up_weight, first_row, group_width, 1)
        down_part = lax.dynamic_slice_in_dim(down_weight, first_row, group_width, 0)
        preact = jnp.maximum(jnp.dot(normed, up_part, preferred_element_type=jnp.float32), 0.0)
        hidden = (preact * preact).astype(jnp.bfloat16)
        partial_value = jnp.dot(hidden, down_part, preferred_element_type=jnp.float32)
        return (running + round_trip(partial_value), None)
    running = jnp.zeros((normed.shape[0], down_weight.shape[1]), jnp.float32)
    running, unused = lax.scan(add_group, running, jnp.arange(groups, dtype=jnp.int32))
    return running

def reference(resid, queries, keys, values, gates, log_decay, retention_output_weight, norm_gain, up_weight, down_weight):
    length = queries.shape[0]
    blocks = length // BLOCK
    token_indices = jnp.arange(length, dtype=jnp.int32)
    query_rot = round_trip(rotate(queries.astype(jnp.float32).reshape(length, HEADS, DK), token_indices))
    key_rot = round_trip(rotate(keys.astype(jnp.float32).reshape(length, HEADS, DK), token_indices) * DK ** (-0.5))
    cumulative = jnp.cumsum(log_decay.astype(jnp.float32).reshape(HEADS, blocks, BLOCK), axis=2)
    per_block = (query_rot.reshape(blocks, BLOCK, HEADS, DK), key_rot.reshape(blocks, BLOCK, HEADS, DK), values.astype(jnp.float32).reshape(blocks, BLOCK, HEADS, DV), gates.astype(jnp.float32).reshape(blocks, BLOCK, HEADS, DV), jnp.moveaxis(cumulative, 1, 0))
    unused, gated_out = lax.scan(block_step, jnp.zeros((HEADS, DK, DV), jnp.float32), per_block)
    gated_out = gated_out.reshape(length, HEADS * DV)
    mixed_sum = grouped_product(gated_out, retention_output_weight, N_TP)
    updated = (resid.astype(jnp.float32) + mixed_sum).astype(jnp.bfloat16)
    normed = normalize(updated, norm_gain)
    channel_sum = channel_mixer(normed, up_weight, down_weight, N_TP)
    return (updated.astype(jnp.float32) + channel_sum).astype(jnp.bfloat16)
```

```python
import functools

import jax
import jax.numpy as jnp
import numpy as np
from jax import lax
from jax.experimental import pallas as pl
from jax.experimental.pallas import tpu as pltpu
from jax.sharding import PartitionSpec as P

DK = 256
DV = 512
BLOCK = 128
SPAN = 256
ROWS = 4
EPS = 1e-06
F32 = jnp.float32
BF16 = jnp.bfloat16
MESH = pl.DeviceIdType.MESH


def dot(a, b):
    return jnp.dot(a, b, preferred_element_type=F32)


def cumulative(row):
    n = row.shape[1]
    i = lax.broadcasted_iota(jnp.int32, (n, n), 0)
    j = lax.broadcasted_iota(jnp.int32, (n, n), 1)
    col = jnp.sum(jnp.where(i == j, row, 0.0), axis=1, keepdims=True)
    cum_col = jnp.sum(jnp.where(j <= i, row, 0.0), axis=1, keepdims=True)
    cum_row = jnp.sum(jnp.where(i <= j, col, 0.0), axis=0, keepdims=True)
    total = jnp.sum(row, axis=1, keepdims=True)
    return i, j, cum_col, cum_row, total


def kernel(
    n_sp, n_tp,
    resid_h, q_h, k_h, v_h, g_h, ld, wo_h, gain, up_h, dn_h, lo_c, lo_s, hi_c, hi_s,
    out,
    q_v, k_v, v_v, g_v, wide, res_v, kr, kd, stf, sth, strun, yst, tot, ytot, crecv, csend, esend, inc, ret,
    pp, pr, psum, xr, acc, upd, x_all, up_all, dn_all, pd, qs, r1, r2y, r2x, r3y, r3x,
    lsem, wsend, wrecv, wysend, wyrecv, ssend, srecv, psend, precv, xsend, xrecv,
    asend, arx, ary, ard, rsend, rrecv,
):
    Z, X = n_sp // 2, n_tp // 2
    sp, tp = lax.axis_index("sp"), lax.axis_index("tp")
    z, y = sp // 2, sp % 2
    x, c = tp // 2, tp % 2
    rows = k_v.shape[0]
    heads = kr.shape[0]
    mine = res_v.shape[0]
    d = res_v.shape[1]
    half = up_all.shape[2]
    cols = dn_all.shape[2]
    nblk, nspan = rows // BLOCK, rows // SPAN
    rc = mine // ROWS
    has_up, has_dn = z < Z - 1, z > 0

    def rcopy(src, dst, ss, rs, dev):
        return pltpu.make_async_remote_copy(src, dst, ss, rs, device_id=dev, device_id_type=MESH)

    to_zp, to_zm = {"sp": sp + 2}, {"sp": sp - 2}
    to_y = {"sp": z * 2 + (1 - y)}
    to_c = {"tp": x * 2 + (1 - c)}

    def xat(j):
        return lax.rem(x + j + X, X)

    def to_x(j):
        return {"tp": xat(j) * 2 + c}

    pending = []

    def send(src, dst, ss, rs, dev, cond=None):
        def go():
            rcopy(src, dst, ss, rs, dev).start()

        def end():
            rcopy(src, dst, ss, rs, dev).wait_send()

        if cond is None:
            go()
        else:
            pl.when(cond)(go)
        pending.append((cond, end))

    def recv(dst, ss, rs):
        rcopy(dst, dst, ss, rs, to_c).wait_recv()

    loads = [
        (k_h, k_v), (v_h, v_v), (q_h, q_v), (g_h, g_v), (resid_h, res_v),
        (up_h.at[:, pl.ds(pl.multiple_of(y * half, half), half)], up_all.at[sp]),
        (dn_h.at[pl.ds(pl.multiple_of(y * half, half), half), :], dn_all.at[sp]),
    ]
    hv = v_v.shape[1]
    stack = wide.shape[0] // hv
    wc = d // stack
    loads += [(wo_h.at[:, pl.ds(i * wc, wc)], wide.at[pl.ds(i * hv, hv)]) for i in range(stack)]

    def load(i):
        return pltpu.make_async_copy(loads[i][0], loads[i][1], lsem.at[i])

    for i in range(len(loads)):
        load(i).start()

    barrier = pltpu.get_barrier_semaphore()
    greet = [(to_y, None), (to_c, None)] + [(to_x(j), None) for j in range(1, X)]
    greet += [(to_zp, has_up), (to_zm, has_dn)]
    for dev, cond in greet:
        def hello(dev=dev):
            pl.semaphore_signal(barrier, 1, device_id=dev, device_id_type=MESH)
        if cond is None:
            hello()
        else:
            pl.when(cond)(hello)
    pl.semaphore_wait(barrier, X + 1 + jnp.where(has_up, 1, 0) + jnp.where(has_dn, 1, 0))

    h_up = up_h.at[:, pl.ds(pl.multiple_of(y * half, half), half)]
    h_dn = dn_h.at[pl.ds(pl.multiple_of(y * half, half), half), :]
    o_up = up_h.at[:, pl.ds(pl.multiple_of((1 - y) * half, half), half)]
    o_dn = dn_h.at[pl.ds(pl.multiple_of((1 - y) * half, half), half), :]
    alls = (up_all, dn_all)

    def zsend(w, piece, src, way):
        dev, cond = ((to_zp, has_up), (to_zm, has_dn))[way]
        send(src, alls[w].at[piece], wsend.at[w, piece, way], wrecv.at[w, piece], dev, cond)

    for w, src in ((0, h_up), (1, h_dn)):
        zsend(w, sp, src, 0)
        zsend(w, sp, src, 1)
    hr = up_h.shape[0] // 2
    other = z * 2 + (1 - y)

    def ysend_up(part):
        at = pl.ds(part * hr, hr)
        send(o_up.at[at], up_all.at[sp, at], wysend.at[part], wyrecv.at[part], to_y)

    ysend_up(0)

    def fwd_y(w, ways=(0, 1), wait=True):
        if wait:
            if w == 0:
                for part in range(2):
                    at = pl.ds(part * hr, hr)
                    recv(up_all.at[other, at], wysend.at[part], wyrecv.at[part])
            else:
                recv(dn_all.at[other], wysend.at[2], wyrecv.at[2])
        for way in ways:
            zsend(w, other, alls[w].at[other], way)

    def fwd(w, k, yy):
        if k > Z - 2:
            return
        low, high = (z - k) * 2 + yy, (z + k) * 2 + yy
        for piece, way, cond in ((low, 0, (z >= k) & has_up), (high, 1, (z + k < Z) & has_dn)):
            dev = (to_zp, to_zm)[way]

            def go(piece=piece, way=way, dev=dev):
                recv(alls[w].at[piece], wsend.at[w, piece, way], wrecv.at[w, piece])
                rcopy(alls[w].at[piece], alls[w].at[piece], wsend.at[w, piece, way], wrecv.at[w, piece], dev).start()

            def end(piece=piece, way=way, dev=dev):
                rcopy(alls[w].at[piece], alls[w].at[piece], wsend.at[w, piece, way], wrecv.at[w, piece], dev).wait_send()

            pl.when(cond)(go)
            pending.append((cond, end))

    def settle(w, piece):
        plane = piece // 2
        cond = ((plane < z) & jnp.logical_not(has_up)) | ((plane > z) & jnp.logical_not(has_dn))

        @pl.when(cond)
        def _():
            recv(alls[w].at[piece], wsend.at[w, piece, 0], wrecv.at[w, piece])

    def angles(b):
        at = sp * nblk + b
        hc, hs = hi_c[pl.ds(at, 1), :], hi_s[pl.ds(at, 1), :]
        lc, ls = lo_c[...], lo_s[...]
        return hc * lc - hs * ls, hs * lc + hc * ls

    def rotated(blk, co, si):
        a, b = blk[:, : DK // 2].astype(F32), blk[:, DK // 2 :].astype(F32)
        return jnp.concatenate([a * co - b * si, a * si + b * co], axis=1)

    tot[...] = jnp.zeros_like(tot)
    load(0).wait()
    for h in range(heads):
        def state_block(t, after, h=h):
            b = nblk - 1 - t
            at = pl.ds(pl.multiple_of(b * BLOCK, BLOCK), BLOCK)
            row = ld[h : h + 1, pl.ds(pl.multiple_of(b * BLOCK, BLOCK), BLOCK)]
            i, j, cum_col, _, total = cumulative(row)
            co, si = angles(b)
            key = (rotated(k_v[at, h * DK : (h + 1) * DK], co, si) * DK ** (-0.5)).astype(BF16)
            kr[h, at, :] = key
            kd[at, :] = (key.astype(F32) * jnp.exp(total - cum_col + after)).astype(BF16)
            return after + total

        whole = lax.fori_loop(0, nblk, state_block, jnp.zeros((1, 1), F32))
        tot[h : h + 1, :] = jnp.broadcast_to(jnp.exp(whole), (1, tot.shape[1]))
        if h == 0:
            load(1).wait()
        s = lax.dot_general(kd[...], v_v[:, h * DV : (h + 1) * DV], (((0,), (0,)), ((), ())), preferred_element_type=F32)
        for p in range(2):
            part = s[:, p * DV // 2 : (p + 1) * DV // 2]
            stf[p, h] = part
            sth[p, h] = part.astype(BF16)
        send(sth.at[1 - y, h], yst.at[h], ssend.at[0, h], srecv.at[0, h], to_y)
    send(tot, ytot, ssend.at[3, 0], srecv.at[3, 0], to_y)
    ysend_up(1)
    send(o_dn, dn_all.at[sp], wysend.at[2], wyrecv.at[2], to_y)

    load(2).wait()

    def local(h):
        strun[...] = jnp.zeros_like(strun)

        def span(t, before):
            at = pl.ds(pl.multiple_of(t * SPAN, SPAN), SPAN)
            row = ld[h : h + 1, pl.ds(pl.multiple_of(t * SPAN, SPAN), SPAN)]
            i, j, cum_col, cum_row, total = cumulative(row)
            parts = []
            for u in range(SPAN // BLOCK):
                co, si = angles(t * (SPAN // BLOCK) + u)
                qat = pl.ds(pl.multiple_of(t * SPAN + u * BLOCK, BLOCK), BLOCK)
                parts.append(rotated(q_v[qat, h * DK : (h + 1) * DK], co, si))
            query = jnp.concatenate(parts, axis=0).astype(BF16)
            key = kr[h, at, :]
            factor = jnp.where(i >= j, jnp.exp(jnp.minimum(cum_col - cum_row, 0.0)), 0.0)
            scores = lax.dot_general(query, key, (((1,), (1,)), ((), ())), preferred_element_type=F32)
            weights = (scores * factor).astype(BF16)
            q32 = query.astype(F32)
            val = v_v[at, h * DV : (h + 1) * DV]
            ret[at, h * DV : (h + 1) * DV] = dot(weights, val) + dot((q32 * jnp.exp(cum_col)).astype(BF16), strun[...].astype(BF16))
            q_v[at, h * DK : (h + 1) * DK] = (q32 * jnp.exp(cum_col + before)).astype(BF16)
            kdec = (key.astype(F32) * jnp.exp(total - cum_col)).astype(BF16)
            strun[...] = jnp.exp(total) * strun[...] + lax.dot_general(
                kdec, val, (((0,), (0,)), ((), ())), preferred_element_type=F32
            )
            return before + total

        lax.fori_loop(0, nspan, span, jnp.zeros((1, 1), F32))

    local(0)

    first = y == 0
    recv(ytot, ssend.at[3, 0], srecv.at[3, 0])

    def decays(h):
        own, oth = tot[h : h + 1, : DV // 2], ytot[h : h + 1, : DV // 2]
        return jnp.where(first, own, oth), jnp.where(first, oth, own)

    @pl.when(jnp.logical_not(has_dn))
    def _():
        crecv[...] = jnp.zeros_like(crecv)

    def combine(h):
        recv(yst.at[h], ssend.at[0, h], srecv.at[0, h])

    def s_pair(h):
        own, oth = stf[y, h], yst[h].astype(F32)
        return jnp.where(first, own, oth), jnp.where(first, oth, own)

    def chain(h):
        d0, d1 = decays(h)
        s0, s1 = s_pair(h)
        csend[h] = (d0 * d1 * crecv[h].astype(F32) + (d1 * s0 + s1)).astype(BF16)

    def chain_send(h):
        rcopy(csend.at[h], crecv.at[h], ssend.at[1, h], srecv.at[1, h], to_zp).start()

    for h in range(heads):
        combine(h)
    @pl.when(jnp.logical_not(has_dn))
    def _():
        for h in range(heads):
            chain(h)
            chain_send(h)

    fwd_y(0, ways=(1,))
    late = z >= 2

    def ou_up():
        rcopy(up_all.at[other], up_all.at[other], wsend.at[0, other, 0], wrecv.at[0, other], to_zp).start()

    pl.when(late & has_up)(ou_up)
    for h in range(1, heads):
        local(h)

    @pl.when(has_dn)
    def _():
        for h in range(heads):
            recv(crecv.at[h], ssend.at[1, h], srecv.at[1, h])

            @pl.when(has_up)
            def _():
                chain(h)
                chain_send(h)

    pl.when(jnp.logical_not(late) & has_up)(ou_up)

    def chain_end():
        for h in range(heads):
            rcopy(csend.at[h], crecv.at[h], ssend.at[1, h], srecv.at[1, h], to_zp).wait_send()
        rcopy(up_all.at[other], up_all.at[other], wsend.at[0, other, 0], wrecv.at[0, other], to_zp).wait_send()

    pending.append((has_up, chain_end))
    for h in range(heads):
        d0, _ = decays(h)
        s0, _ = s_pair(h)
        got = crecv[h].astype(F32)
        later = (d0 * got + s0).astype(BF16)
        inc[y, h] = jnp.where(first, crecv[h], later)
        esend[h] = jnp.where(first, later, crecv[h])
        send(esend.at[h], inc.at[y, h], ssend.at[2, h], srecv.at[2, h], to_y)
    fwd(0, 1, y)
    fwd_y(1)
    load(3).wait()
    for i in range(stack):
        load(7 + i).wait()
    for h in range(heads):
        recv(inc.at[1 - y, h], ssend.at[2, h], srecv.at[2, h])

    fr = min(128, mine)

    def finish(owner):
        base = owner * mine

        def part(t, carry):
            at = pl.ds(pl.multiple_of(base + t * fr, fr), fr)
            for h in range(heads):
                qd = q_v[at, h * DK : (h + 1) * DK]
                r = ret[at, h * DV : (h + 1) * DV] + jnp.concatenate([dot(qd, inc[0, h]), dot(qd, inc[1, h])], axis=1)
                normed = r * lax.rsqrt(jnp.mean(r * r, axis=1, keepdims=True) + EPS)
                g = g_v[at, h * DV : (h + 1) * DV].astype(F32)
                g_v[at, h * DV : (h + 1) * DV] = (g / (1.0 + jnp.exp(-g)) * normed).astype(BF16)
            return carry

        lax.fori_loop(0, mine // fr, part, 0)

    pt = min(512, wc)

    def project(owner, put):
        rows_at = pl.ds(pl.multiple_of(owner * mine, mine), mine)
        for i in range(stack):
            def part(t, carry, i=i):
                at = pl.ds(pl.multiple_of(t * pt, pt), pt)
                to = pl.ds(pl.multiple_of(i * wc + t * pt, pt), pt)
                put(to, dot(g_v[rows_at, :], wide[i * hv : (i + 1) * hv, at]))
                return carry

            lax.fori_loop(0, wc // pt, part, 0)

    def for_sibling(j):
        owner = xat(j) * 2 + (1 - c)
        finish(owner)

        def put(at, val):
            pp[j, :, at] = val.astype(BF16)

        project(owner, put)
        send(pp.at[j], pr.at[j], psend.at[j], precv.at[j], to_c)

    def for_mine(j):
        owner = xat(j) * 2 + c
        finish(owner)

        def put(at, val):
            acc[:, at] = val.astype(BF16).astype(F32)

        project(owner, put)
        recv(pr.at[j], psend.at[j], precv.at[j])
        if j:
            for r in range(ROWS):
                at = pl.ds(r * rc, rc)
                psum[j - 1, at, :] = (acc[at, :] + pr[j, at, :].astype(F32)).astype(BF16)
                send(psum.at[j - 1, at], xr.at[j - 1, at], xsend.at[j - 1, r], xrecv.at[j - 1, r], to_x(j))

    for j in range(1, X):
        for_sibling(j)
        for_mine(j)
    fwd(0, 1, 1 - y)
    for_sibling(0)
    for_mine(0)
    fwd(0, 2, y)

    load(4).wait()
    for r in range(ROWS):
        at = pl.ds(r * rc, rc)
        s = acc[at, :] + pr[0, at, :].astype(F32)
        for j in range(1, X):
            recv(xr.at[j - 1, at], xsend.at[j - 1, r], xrecv.at[j - 1, r])
            s = s + xr[j - 1, at, :].astype(F32)
        u = (res_v[at, :].astype(F32) + s).astype(BF16)
        upd[at, :] = u
        u = u.astype(F32)
        u = u * lax.rsqrt(jnp.mean(u * u, axis=1, keepdims=True) + EPS)
        x_all[c, y, x, at, :] = (u * gain[...].astype(F32)).astype(BF16)
        own = x_all.at[c, y, x, at]
        send(own, own, asend.at[0, 0, r], ary.at[0, r], to_y)
        for j in range(1, X):
            send(own, own, asend.at[1, j, r], arx.at[j, r], to_x(j))
        send(own, own, asend.at[2, 0, r], ard.at[0, 0, r], to_c)

    load(5).wait()
    for k in range(1, Z - 1):
        if k == 1:
            continue
        fwd(0, k, 1 - y)
        if k > 2:
            fwd(0, k, y)

    for k in range(n_sp):
        settle(0, k)

    ht = min(512, half)

    def hid_rows(yy, xx):
        return pl.ds(pl.multiple_of((yy * X + xx) * mine, mine), mine)

    def hid_of(cc):
        return pl.ds(pl.multiple_of(cc * half, half), half)

    def hidden(yy, xx):
        def part(t, carry):
            at = pl.ds(pl.multiple_of(t * ht, ht), ht)
            w = up_all[:, :, at].reshape(d, ht)
            for cc in range(2):
                pre = jnp.maximum(dot(x_all[cc, yy, xx], w), 0.0)
                col = pl.ds(pl.multiple_of(cc * half + t * ht, ht), ht)
                wide[hid_rows(yy, xx), col] = (pre * pre).astype(BF16)
            return carry

        lax.fori_loop(0, half // ht, part, 0)

    def from_sibling(yrel, i, r):
        at = pl.ds(r * rc, rc)
        dst = x_all.at[1 - c, jnp.where(yrel == 0, y, 1 - y), xat(-i), at]
        recv(dst, asend.at[2, 0, r], ard.at[yrel, i, r])

    def pass_on(yrel, i, r):
        at = pl.ds(r * rc, rc)
        ref = x_all.at[c, (1 - y) if yrel else y, xat(-i), at]
        if yrel:
            recv(ref, asend.at[0, 0, r], ary.at[i, r])
        else:
            recv(ref, asend.at[1, i, r], arx.at[i, r])
            send(ref, ref, asend.at[0, i, r], ary.at[i, r], to_y)
        send(ref, ref, asend.at[2 + yrel, i, r], ard.at[yrel, i, r], to_c)

    for r in range(ROWS):
        from_sibling(0, 0, r)
    hidden(y, x)
    for r in range(ROWS):
        pass_on(1, 0, r)
        for j in range(1, X):
            pass_on(0, j, r)
        if r == 1:
            fwd(1, 1, 0)
            fwd(1, 1, 1)
    for r in range(ROWS):
        from_sibling(1, 0, r)
    hidden(1 - y, x)
    for k in range(2, Z - 1):
        fwd(1, k, 0)
        fwd(1, k, 1)
    for j in range(1, X):
        for r in range(ROWS):
            from_sibling(0, j, r)
        hidden(y, xat(-j))
    for j in range(1, X):
        for r in range(ROWS):
            pass_on(1, j, r)
        for r in range(ROWS):
            from_sibling(1, j, r)
        hidden(1 - y, xat(-j))

    load(6).wait()
    m = jnp.minimum(z, Z - 1 - z)
    hm = mine // 2

    def block_of(s):
        i = s // 2
        near = jnp.where(i % 2 == 1, z - (i + 1) // 2, z + i // 2)
        far = jnp.where(z <= Z - 1 - z, i, Z - 1 - i)
        return jnp.where(i <= 2 * m, near, far) * 2 + s % 2

    def to_sib(s):
        return rcopy(pd.at[s % 2], r1.at[s], rsend.at[0, s], rrecv.at[0, s], to_c)

    def a_y(s):
        return rcopy(qs.at[s % 4, 1 - y, :, 0], r2y.at[s], rsend.at[1, s], rrecv.at[1, s], to_y)

    def a_x(s, j):
        return rcopy(qs.at[s % 4, :, xat(j), 1], r2x.at[s, j - 1], rsend.at[3 + j, s], rrecv.at[3 + j, s], to_x(j))

    def b_y(s):
        return rcopy(qs.at[s % 4, 1 - y, x, 1], r3y.at[s], rsend.at[2, s], rrecv.at[2, s], to_y)

    def b_x(s, j):
        return rcopy(qs.at[s % 4, y, xat(j), 0], r3x.at[s, j - 1], rsend.at[3 + X + j, s], rrecv.at[3 + X + j, s], to_x(j))

    def step(s, carry):
        @pl.when(s < n_sp)
        def _():
            u = block_of(s)
            settle(1, u)

            @pl.when(s >= 2)
            def _():
                to_sib(s - 2).wait_send()

            w = dn_all[u]
            for yy in range(2):
                for xx in range(X):
                    pd[s % 2, yy, xx] = dot(wide[hid_rows(yy, xx), hid_of(1 - c)], w).astype(BF16).reshape(2, hm, cols)
            to_sib(s).start()
            for yy in range(2):
                for xx in range(X):
                    ret[hid_rows(yy, xx), :cols] = dot(wide[hid_rows(yy, xx), hid_of(c)], w)

        @pl.when((s >= 1) & (s <= n_sp))
        def _():
            p = s - 1
            a_y(p).wait_recv()
            qs[p % 4, y, :, 0] = (qs[p % 4, y, :, 0].astype(F32) + r2y[p].astype(F32)).astype(BF16)
            t = qs[p % 4, :, x, 1].astype(F32)
            for j in range(1, X):
                a_x(p, j).wait_recv()
                t = t + r2x[p, j - 1].astype(F32)
            qs[p % 4, :, x, 1] = t.astype(BF16)
            b_y(p).start()
            for j in range(1, X):
                b_x(p, j).start()

        @pl.when(s < n_sp)
        def _():
            to_sib(s).wait_recv()
            own = ret[: 2 * X * mine, :cols].reshape(2, X, 2, hm, cols)
            qs[s % 4] = (own.astype(BF16).astype(F32) + r1[s].astype(F32)).astype(BF16)
            a_y(s).start()
            for j in range(1, X):
                a_x(s, j).start()

        @pl.when(s >= 2)
        def _():
            p = s - 2
            u = block_of(p)
            at = pl.ds(pl.multiple_of(u * cols, cols), cols)
            t = upd[:hm, at].astype(F32) + qs[p % 4, y, x, 0].astype(F32)
            for j in range(1, X):
                b_x(p, j).wait_recv()
                t = t + r3x[p, j - 1].astype(F32)
            out[:hm, at] = t.astype(BF16)
            b_y(p).wait_recv()
            t = upd[hm:, at].astype(F32) + qs[p % 4, y, x, 1].astype(F32) + r3y[p].astype(F32)
            out[hm:, at] = t.astype(BF16)
            a_y(p).wait_send()
            b_y(p).wait_send()
            for j in range(1, X):
                a_x(p, j).wait_send()
                b_x(p, j).wait_send()

        return carry

    lax.fori_loop(0, n_sp + 2, step, 0)
    for s in (n_sp - 2, n_sp - 1):
        to_sib(s).wait_send()
    for cond, end in pending:
        if cond is None:
            end()
        else:
            pl.when(cond)(end)


def body(n_sp, n_tp, resid, queries, keys, values, gates, log_decay, w_out, gain, up, down):
    X, Z = n_tp // 2, n_sp // 2
    rows, heads = queries.shape[0], log_decay.shape[0]
    mine, d = resid.shape
    half, cols, part = up.shape[1] // 2, down.shape[1], up.shape[0]
    freq = 10000.0 ** (-np.arange(0, DK, 2, dtype=np.float64) / DK)
    low = np.arange(BLOCK)[:, None] * freq[None, :]
    high = (BLOCK * np.arange(rows * n_sp // BLOCK))[:, None] * freq[None, :]
    tables = [jnp.asarray(f(a), F32) for a in (low, high) for f in (np.cos, np.sin)]
    vm, anym = pl.BlockSpec(memory_space=pltpu.VMEM), pl.BlockSpec(memory_space=pl.ANY)
    dma = pltpu.SemaphoreType.DMA
    V = pltpu.VMEM
    hd, hv = heads * DK, heads * DV
    sq = (DK, DV // 2)
    scratch = [
        V((rows, hd), BF16), V((rows, hd), BF16), V((rows, hv), BF16), V((rows, hv), BF16),
        V((2 * X * mine, 2 * half), BF16), V((mine, d), BF16),
        V((heads, rows, DK), BF16), V((rows, DK), BF16),
        V((2, heads, *sq), F32), V((2, heads, *sq), BF16), V((DK, DV), F32),
        V((heads, *sq), BF16), V((8, DV // 2), F32), V((8, DV // 2), F32),
        V((heads, *sq), BF16), V((heads, *sq), BF16), V((heads, *sq), BF16), V((2, heads, *sq), BF16),
        V((rows, hv), F32),
        V((X, mine, d), BF16), V((X, mine, d), BF16), V((X - 1, mine, d), BF16), V((X - 1, mine, d), BF16),
        V((mine, d), F32), V((mine, d), BF16),
        V((2, 2, X, mine, d), BF16), V((n_sp, part, half), BF16), V((n_sp, half, cols), BF16),
        V((2, 2, X, 2, mine // 2, cols), BF16),
        V((4, 2, X, 2, mine // 2, cols), BF16), V((n_sp, 2, X, 2, mine // 2, cols), BF16),
        V((n_sp, X, mine // 2, cols), BF16), V((n_sp, X - 1, 2, mine // 2, cols), BF16),
        V((n_sp, mine // 2, cols), BF16), V((n_sp, X - 1, mine // 2, cols), BF16),
        dma((7 + 2 * X * mine // hv,)), dma((2, n_sp, 2)), dma((2, n_sp)), dma((3,)), dma((3,)),
        dma((4, heads)), dma((4, heads)), dma((X,)), dma((X,)), dma((X, ROWS)), dma((X, ROWS)),
        dma((4, X, ROWS)), dma((X, ROWS)), dma((X, ROWS)), dma((2, X, ROWS)),
        dma((4 + 2 * X, n_sp)), dma((4 + 2 * X, n_sp)),
    ]
    return pl.pallas_call(
        functools.partial(kernel, n_sp, n_tp),
        in_specs=[anym] * 5 + [vm, anym, vm, anym, anym] + [vm] * 4,
        out_specs=vm,
        out_shape=jax.ShapeDtypeStruct((mine, d), BF16),
        scratch_shapes=scratch,
        compiler_params=pltpu.CompilerParams(
            collective_id=0, has_side_effects=True, vmem_limit_bytes=67043328
        ),
        name="layer",
    )(resid, queries, keys, values, gates, log_decay, w_out, gain.reshape(1, d), up, down, *tables)


def solution(mesh):
    placed = (
        P(("sp", "tp"), None),
        P("sp", "tp"),
        P("sp", "tp"),
        P("sp", "tp"),
        P("sp", "tp"),
        P("tp", "sp"),
        P("tp", None),
        P(),
        P("sp", "tp"),
        P("tp", "sp"),
    )
    return jax.shard_map(
        functools.partial(body, mesh.shape["sp"], mesh.shape["tp"]),
        mesh=mesh,
        in_specs=placed,
        out_specs=P(("sp", "tp"), None),
        check_vma=False,
    )
```

```python
import functools

import jax
import jax.numpy as jnp
import numpy as np
from jax import lax
from jax.experimental import pallas as pl
from jax.experimental.pallas import tpu as pltpu
from jax.sharding import PartitionSpec as P

DK = 256
DV = 512
BLOCK = 128
SPAN = 256
ROWS = 4
SLOTS = 6
EPS = 1e-06
F32 = jnp.float32
BF16 = jnp.bfloat16
MESH = pl.DeviceIdType.MESH


def dot(a, b):
    return jnp.dot(a, b, preferred_element_type=F32)


def cumulative(row):
    n = row.shape[1]
    i = lax.broadcasted_iota(jnp.int32, (n, n), 0)
    j = lax.broadcasted_iota(jnp.int32, (n, n), 1)
    col = jnp.sum(jnp.where(i == j, row, 0.0), axis=1, keepdims=True)
    cum_col = jnp.sum(jnp.where(j <= i, row, 0.0), axis=1, keepdims=True)
    cum_row = jnp.sum(jnp.where(i <= j, col, 0.0), axis=0, keepdims=True)
    total = jnp.sum(row, axis=1, keepdims=True)
    return i, j, cum_col, cum_row, total


def kernel(
    n_sp, n_tp,
    resid_h, q_h, k_h, v_h, g_h, ld, wo_h, gain, up_h, dn_h, lo_c, lo_s, hi_c, hi_s,
    out,
    q_v, k_v, v_v, g_v, wide, res_v, kr, kd, stf, sth, strun, yst, tot, ytot, crecv, csend, esend, inc, ret,
    pp, pr, psum, xr, acc, upd, x_all, up_all, dn_all, pd, qs, r1, r2y, r2x, r3y, r3x,
    lsem, wsend, wrecv, wysend, wyrecv, ssend, srecv, psend, precv, xsend, xrecv,
    asend, arx, ary, ard, rsend, rrecv,
):
    Z, X = n_sp // 2, n_tp // 2
    sp, tp = lax.axis_index("sp"), lax.axis_index("tp")
    z, y = sp // 2, sp % 2
    x, c = tp // 2, tp % 2
    rows = k_v.shape[0]
    heads = kr.shape[0]
    mine = res_v.shape[0]
    d = res_v.shape[1]
    half = up_all.shape[2]
    cols = dn_all.shape[2]
    nblk, nspan = rows // BLOCK, rows // SPAN
    rc = mine // ROWS
    has_up, has_dn = z < Z - 1, z > 0

    def rcopy(src, dst, ss, rs, dev):
        return pltpu.make_async_remote_copy(src, dst, ss, rs, device_id=dev, device_id_type=MESH)

    to_zp, to_zm = {"sp": sp + 2}, {"sp": sp - 2}
    to_y = {"sp": z * 2 + (1 - y)}
    to_c = {"tp": x * 2 + (1 - c)}

    def xat(j):
        return lax.rem(x + j + X, X)

    def to_x(j):
        return {"tp": xat(j) * 2 + c}

    pending = []

    def send(src, dst, ss, rs, dev, cond=None):
        def go():
            rcopy(src, dst, ss, rs, dev).start()

        def end():
            rcopy(src, dst, ss, rs, dev).wait_send()

        if cond is None:
            go()
        else:
            pl.when(cond)(go)
        pending.append((cond, end))

    def recv(dst, ss, rs):
        rcopy(dst, dst, ss, rs, to_c).wait_recv()

    loads = [
        (k_h, k_v), (v_h, v_v), (q_h, q_v), (g_h, g_v), (resid_h, res_v),
        (up_h.at[:, pl.ds(pl.multiple_of(y * half, half), half)], up_all.at[sp]),
        (dn_h.at[pl.ds(pl.multiple_of(y * half, half), half), :], dn_all.at[sp]),
    ]
    hv = v_v.shape[1]
    stack = wide.shape[0] // hv
    wc = d // stack
    loads += [(wo_h.at[:, pl.ds(i * wc, wc)], wide.at[pl.ds(i * hv, hv)]) for i in range(stack)]

    def load(i):
        return pltpu.make_async_copy(loads[i][0], loads[i][1], lsem.at[i])

    for i in range(len(loads)):
        load(i).start()

    barrier = pltpu.get_barrier_semaphore()
    greet = [(to_y, None), (to_c, None)] + [(to_x(j), None) for j in range(1, X)]
    greet += [(to_zp, has_up), (to_zm, has_dn)]
    for dev, cond in greet:
        def hello(dev=dev):
            pl.semaphore_signal(barrier, 1, device_id=dev, device_id_type=MESH)
        if cond is None:
            hello()
        else:
            pl.when(cond)(hello)
    pl.semaphore_wait(barrier, X + 1 + jnp.where(has_up, 1, 0) + jnp.where(has_dn, 1, 0))

    h_up = up_h.at[:, pl.ds(pl.multiple_of(y * half, half), half)]
    h_dn = dn_h.at[pl.ds(pl.multiple_of(y * half, half), half), :]
    o_up = up_h.at[:, pl.ds(pl.multiple_of((1 - y) * half, half), half)]
    o_dn = dn_h.at[pl.ds(pl.multiple_of((1 - y) * half, half), half), :]
    alls = (up_all, dn_all)

    def zsend(w, piece, src, way):
        dev, cond = ((to_zp, has_up), (to_zm, has_dn))[way]
        send(src, alls[w].at[piece], wsend.at[w, piece, way], wrecv.at[w, piece], dev, cond)

    late = z >= 2
    early = jnp.logical_not(late)
    for way in range(2):
        zsend(0, sp, h_up, way)
    zsend(1, sp, h_dn, 1)

    def own_dn():
        return rcopy(h_dn, dn_all.at[sp], wsend.at[1, sp, 0], wrecv.at[1, sp], to_zp)

    @pl.when(late & has_up)
    def _():
        own_dn().start()

    pending.append((has_up, lambda: own_dn().wait_send()))
    hr = up_h.shape[0] // 2
    other = z * 2 + (1 - y)

    def ysend(w, src):
        send(src, alls[w].at[sp], wysend.at[w], wyrecv.at[w], to_y)

    def recv_y(w):
        recv(alls[w].at[other], wysend.at[w], wyrecv.at[w])

    def relays(w, k, yy):
        parts = []
        low, high = (z - k) * 2 + yy, (z + k) * 2 + yy
        for piece, way, cond in ((low, 0, (z >= k) & has_up), (high, 1, (z + k < Z) & has_dn)):
            def copy(piece=piece, way=way):
                ref = alls[w].at[piece]
                return rcopy(ref, ref, wsend.at[w, piece, way], wrecv.at[w, piece], (to_zp, to_zm)[way])

            def go(copy=copy):
                copy().wait_recv()
                copy().start()

            pending.append((cond, lambda copy=copy: copy().wait_send()))
            parts.append((cond, go))
        return parts

    def fwd(w, k, yy):
        if k <= Z - 2:
            for cond, go in relays(w, k, yy):
                pl.when(cond)(go)

    def settle(w, piece):
        plane = piece // 2
        cond = ((plane < z) & jnp.logical_not(has_up)) | ((plane > z) & jnp.logical_not(has_dn))

        @pl.when(cond)
        def _():
            recv(alls[w].at[piece], wsend.at[w, piece, 0], wrecv.at[w, piece])

    def angles(b):
        at = sp * nblk + b
        hc, hs = hi_c[pl.ds(at, 1), :], hi_s[pl.ds(at, 1), :]
        lc, ls = lo_c[...], lo_s[...]
        return hc * lc - hs * ls, hs * lc + hc * ls

    def rotated(blk, co, si):
        a, b = blk[:, : DK // 2].astype(F32), blk[:, DK // 2 :].astype(F32)
        return jnp.concatenate([a * co - b * si, a * si + b * co], axis=1)

    tot[...] = jnp.zeros_like(tot)
    load(0).wait()
    for h in range(heads):
        def state_block(t, after, h=h):
            b = nblk - 1 - t
            at = pl.ds(pl.multiple_of(b * BLOCK, BLOCK), BLOCK)
            row = ld[h : h + 1, pl.ds(pl.multiple_of(b * BLOCK, BLOCK), BLOCK)]
            i, j, cum_col, _, total = cumulative(row)
            co, si = angles(b)
            key = (rotated(k_v[at, h * DK : (h + 1) * DK], co, si) * DK ** (-0.5)).astype(BF16)
            kr[h, at, :] = key
            kd[at, :] = (key.astype(F32) * jnp.exp(total - cum_col + after)).astype(BF16)
            return after + total

        whole = lax.fori_loop(0, nblk, state_block, jnp.zeros((1, 1), F32))
        tot[h : h + 1, :] = jnp.broadcast_to(jnp.exp(whole), (1, tot.shape[1]))
        if h == 0:
            load(1).wait()
        s = lax.dot_general(kd[...], v_v[:, h * DV : (h + 1) * DV], (((0,), (0,)), ((), ())), preferred_element_type=F32)
        for p in range(2):
            part = s[:, p * DV // 2 : (p + 1) * DV // 2]
            stf[p, h] = part
            sth[p, h] = part.astype(BF16)
        send(sth.at[1 - y, h], yst.at[h], ssend.at[0, h], srecv.at[0, h], to_y)
    send(tot, ytot, ssend.at[3, 0], srecv.at[3, 0], to_y)
    ysend(0, o_up)
    ysend(1, o_dn)

    load(2).wait()

    def local(h):
        strun[...] = jnp.zeros_like(strun)

        def span(t, before):
            at = pl.ds(pl.multiple_of(t * SPAN, SPAN), SPAN)
            row = ld[h : h + 1, pl.ds(pl.multiple_of(t * SPAN, SPAN), SPAN)]
            i, j, cum_col, cum_row, total = cumulative(row)
            parts = []
            for u in range(SPAN // BLOCK):
                co, si = angles(t * (SPAN // BLOCK) + u)
                qat = pl.ds(pl.multiple_of(t * SPAN + u * BLOCK, BLOCK), BLOCK)
                parts.append(rotated(q_v[qat, h * DK : (h + 1) * DK], co, si))
            query = jnp.concatenate(parts, axis=0).astype(BF16)
            key = kr[h, at, :]
            factor = jnp.where(i >= j, jnp.exp(jnp.minimum(cum_col - cum_row, 0.0)), 0.0)
            scores = lax.dot_general(query, key, (((1,), (1,)), ((), ())), preferred_element_type=F32)
            weights = (scores * factor).astype(BF16)
            q32 = query.astype(F32)
            val = v_v[at, h * DV : (h + 1) * DV]
            ret[at, h * DV : (h + 1) * DV] = dot(weights, val) + dot((q32 * jnp.exp(cum_col)).astype(BF16), strun[...].astype(BF16))
            q_v[at, h * DK : (h + 1) * DK] = (q32 * jnp.exp(cum_col + before)).astype(BF16)
            kdec = (key.astype(F32) * jnp.exp(total - cum_col)).astype(BF16)
            strun[...] = jnp.exp(total) * strun[...] + lax.dot_general(
                kdec, val, (((0,), (0,)), ((), ())), preferred_element_type=F32
            )
            return before + total

        lax.fori_loop(0, nspan, span, jnp.zeros((1, 1), F32))

    local(0)

    first = y == 0
    recv(ytot, ssend.at[3, 0], srecv.at[3, 0])

    def decays(h):
        own, oth = tot[h : h + 1, : DV // 2], ytot[h : h + 1, : DV // 2]
        return jnp.where(first, own, oth), jnp.where(first, oth, own)

    @pl.when(jnp.logical_not(has_dn))
    def _():
        crecv[...] = jnp.zeros_like(crecv)

    def combine(h):
        recv(yst.at[h], ssend.at[0, h], srecv.at[0, h])

    def s_pair(h):
        own, oth = stf[y, h], yst[h].astype(F32)
        return jnp.where(first, own, oth), jnp.where(first, oth, own)

    def chain(h):
        d0, d1 = decays(h)
        s0, s1 = s_pair(h)
        csend[h] = (d0 * d1 * crecv[h].astype(F32) + (d1 * s0 + s1)).astype(BF16)

    def chain_send(h):
        rcopy(csend.at[h], crecv.at[h], ssend.at[1, h], srecv.at[1, h], to_zp).start()

    for h in range(heads):
        combine(h)
    @pl.when(jnp.logical_not(has_dn))
    def _():
        for h in range(heads):
            chain(h)
            chain_send(h)
        own_dn().start()

    for h in range(1, heads):
        local(h)

    def part_up(part):
        ref = up_all.at[other, pl.ds(part * hr, hr)]
        rcopy(ref, ref, wsend.at[0, other, 0], wrecv.at[0, other], to_zp).start()

    @pl.when(late)
    def _():
        recv_y(0)
        pl.when(has_up)(lambda: part_up(0))

    @pl.when(has_dn)
    def _():
        for h in range(heads):
            recv(crecv.at[h], ssend.at[1, h], srecv.at[1, h])

            @pl.when(has_up)
            def _():
                chain(h)
                chain_send(h)

        @pl.when(early & has_up)
        def _():
            own_dn().start()

    def chain_end():
        for h in range(heads):
            rcopy(csend.at[h], crecv.at[h], ssend.at[1, h], srecv.at[1, h], to_zp).wait_send()
        rcopy(up_all.at[other], up_all.at[other], wsend.at[0, other, 0], wrecv.at[0, other], to_zp).wait_send()

    pending.append((has_up, chain_end))
    for h in range(heads):
        d0, _ = decays(h)
        s0, _ = s_pair(h)
        got = crecv[h].astype(F32)
        later = (d0 * got + s0).astype(BF16)
        inc[y, h] = jnp.where(first, crecv[h], later)
        esend[h] = jnp.where(first, later, crecv[h])
        send(esend.at[h], inc.at[y, h], ssend.at[2, h], srecv.at[2, h], to_y)
    @pl.when(early)
    def _():
        recv_y(0)
        pl.when(has_up)(lambda: part_up(0))

    pl.when(has_up)(lambda: part_up(1))
    zsend(0, other, up_all.at[other], 1)
    fwd(0, 1, y)
    load(3).wait()
    for i in range(stack):
        load(7 + i).wait()
    for h in range(heads):
        recv(inc.at[1 - y, h], ssend.at[2, h], srecv.at[2, h])

    ph = mine // 2
    fr = min(128, ph)

    def finish(base):

        def part(t, carry):
            at = pl.ds(pl.multiple_of(base + t * fr, fr), fr)
            for h in range(heads):
                qd = q_v[at, h * DK : (h + 1) * DK]
                r = ret[at, h * DV : (h + 1) * DV] + jnp.concatenate([dot(qd, inc[0, h]), dot(qd, inc[1, h])], axis=1)
                normed = r * lax.rsqrt(jnp.mean(r * r, axis=1, keepdims=True) + EPS)
                g = g_v[at, h * DV : (h + 1) * DV].astype(F32)
                g_v[at, h * DV : (h + 1) * DV] = (g / (1.0 + jnp.exp(-g)) * normed).astype(BF16)
            return carry

        lax.fori_loop(0, ph // fr, part, 0)

    pt = min(512, wc)

    def project(base, put):
        rows_at = pl.ds(pl.multiple_of(base, ph), ph)
        for i in range(stack):
            def part(t, carry, i=i):
                at = pl.ds(pl.multiple_of(t * pt, pt), pt)
                to = pl.ds(pl.multiple_of(i * wc + t * pt, pt), pt)
                put(to, dot(g_v[rows_at, :], wide[i * hv : (i + 1) * hv, at]))
                return carry

            lax.fori_loop(0, wc // pt, part, 0)

    def for_sibling(j, p):
        base = (xat(j) * 2 + (1 - c)) * mine + p * ph
        finish(base)
        mid = pl.ds(p * ph, ph)

        def put(at, val):
            pp[j, mid, at] = val.astype(BF16)

        project(base, put)
        send(pp.at[j, mid], pr.at[j, mid], psend.at[j, p], precv.at[j, p], to_c)

    def for_mine(j, p):
        base = (xat(j) * 2 + c) * mine + p * ph
        finish(base)
        mid = pl.ds(p * ph, ph)

        def put(at, val):
            acc[mid, at] = val.astype(BF16).astype(F32)

        project(base, put)
        recv(pr.at[j, mid], psend.at[j, p], precv.at[j, p])
        if j:
            for r in range(p * ROWS // 2, (p + 1) * ROWS // 2):
                at = pl.ds(r * rc, rc)
                psum[j - 1, at, :] = (acc[at, :] + pr[j, at, :].astype(F32)).astype(BF16)
                send(psum.at[j - 1, at], xr.at[j - 1, at], xsend.at[j - 1, r], xrecv.at[j - 1, r], to_x(j))

    for j in range(1, X):
        for p in range(2):
            for_sibling(j, p)
            for_mine(j, p)
    fwd(0, 1, 1 - y)
    for p in range(2):
        for_sibling(0, p)
        for_mine(0, p)
    recv_y(1)
    for way in range(2):
        zsend(1, other, dn_all.at[other], way)
    fwd(0, 2, y)

    load(4).wait()
    for r in range(ROWS):
        at = pl.ds(r * rc, rc)
        s = acc[at, :] + pr[0, at, :].astype(F32)
        for j in range(1, X):
            recv(xr.at[j - 1, at], xsend.at[j - 1, r], xrecv.at[j - 1, r])
            s = s + xr[j - 1, at, :].astype(F32)
        u = (res_v[at, :].astype(F32) + s).astype(BF16)
        upd[at, :] = u
        u = u.astype(F32)
        u = u * lax.rsqrt(jnp.mean(u * u, axis=1, keepdims=True) + EPS)
        x_all[c, y, x, at, :] = (u * gain[...].astype(F32)).astype(BF16)
        own = x_all.at[c, y, x, at]
        send(own, own, asend.at[0, 0, r], ary.at[0, r], to_y)
        for j in range(1, X):
            send(own, own, asend.at[1, j, r], arx.at[j, r], to_x(j))
        send(own, own, asend.at[2, 0, r], ard.at[0, 0, r], to_c)

    load(5).wait()
    for k in range(1, Z - 1):
        if k == 1:
            continue
        fwd(0, k, 1 - y)
        if k > 2:
            fwd(0, k, y)

    ht = min(512, half)

    def hid_rows(yy, xx):
        return pl.ds(pl.multiple_of((yy * X + xx) * mine, mine), mine)

    def hid_of(cc):
        return pl.ds(pl.multiple_of(cc * half, half), half)

    def hidden(yy, xx):
        def part(t, carry):
            at = pl.ds(pl.multiple_of(t * ht, ht), ht)
            w = up_all[:, :, at].reshape(d, ht)
            for cc in range(2):
                pre = jnp.maximum(dot(x_all[cc, yy, xx], w), 0.0)
                col = pl.ds(pl.multiple_of(cc * half + t * ht, ht), ht)
                wide[hid_rows(yy, xx), col] = (pre * pre).astype(BF16)
            return carry

        lax.fori_loop(0, half // ht, part, 0)

    def from_sibling(yrel, i, r):
        at = pl.ds(r * rc, rc)
        dst = x_all.at[1 - c, jnp.where(yrel == 0, y, 1 - y), xat(-i), at]
        recv(dst, asend.at[2, 0, r], ard.at[yrel, i, r])

    def pass_on(yrel, i, r):
        at = pl.ds(r * rc, rc)
        ref = x_all.at[c, (1 - y) if yrel else y, xat(-i), at]
        if yrel:
            recv(ref, asend.at[0, 0, r], ary.at[i, r])
        else:
            recv(ref, asend.at[1, i, r], arx.at[i, r])
            send(ref, ref, asend.at[0, i, r], ary.at[i, r], to_y)
        send(ref, ref, asend.at[2 + yrel, i, r], ard.at[yrel, i, r], to_c)

    for r in range(ROWS):
        pass_on(1, 0, r)
    for r in range(ROWS):
        for j in range(1, X):
            pass_on(0, j, r)
        if r == 1:
            fwd(1, 1, 0)
    fwd(1, 1, 1)
    for k in range(n_sp):
        settle(0, k)
    for r in range(ROWS):
        from_sibling(0, 0, r)
    hidden(y, x)
    for r in range(ROWS):
        from_sibling(1, 0, r)
    hidden(1 - y, x)
    for j in range(1, X):
        for r in range(ROWS):
            pass_on(1, j, r)
        for r in range(ROWS):
            from_sibling(0, j, r)
        hidden(y, xat(-j))
    for j in range(1, X):
        for r in range(ROWS):
            from_sibling(1, j, r)
        hidden(1 - y, xat(-j))

    load(6).wait()
    m = jnp.minimum(z, Z - 1 - z)
    hm = mine // 2

    def block_of(s):
        i = s // 2
        near = jnp.where(i % 2 == 1, z - (i + 1) // 2, z + i // 2)
        far = jnp.where(z <= Z - 1 - z, i, Z - 1 - i)
        return jnp.where(i <= 2 * m, near, far) * 2 + s % 2

    def to_sib(s):
        return rcopy(pd.at[s % 2], r1.at[s], rsend.at[0, s], rrecv.at[0, s], to_c)

    def a_y(s):
        return rcopy(qs.at[s % SLOTS, 1 - y, :, 0], r2y.at[s], rsend.at[1, s], rrecv.at[1, s], to_y)

    def a_x(s, j):
        return rcopy(qs.at[s % SLOTS, :, xat(j), 1], r2x.at[s, j - 1], rsend.at[3 + j, s], rrecv.at[3 + j, s], to_x(j))

    def b_y(s):
        return rcopy(qs.at[s % SLOTS, 1 - y, x, 1], r3y.at[s], rsend.at[2, s], rrecv.at[2, s], to_y)

    def b_x(s, j):
        return rcopy(qs.at[s % SLOTS, y, xat(j), 0], r3x.at[s, j - 1], rsend.at[3 + X + j, s], rrecv.at[3 + X + j, s], to_x(j))

    last = [(2 * (k - 2 + yy), relays(1, k, yy)) for k in range(2, Z - 1) for yy in range(2)]

    def step(s, carry):
        for at, parts in last:
            for cond, go in parts:
                pl.when(cond & (s == at))(go)

        @pl.when(s < n_sp)
        def _():
            u = block_of(s)
            settle(1, u)

            @pl.when(s >= 2)
            def _():
                to_sib(s - 2).wait_send()

            w = dn_all[u]
            pd[s % 2] = dot(wide[:, hid_of(1 - c)], w).astype(BF16).reshape(2, X, 2, hm, cols)
            to_sib(s).start()
            ret[: 2 * X * mine, :cols] = dot(wide[:, hid_of(c)], w)

        @pl.when((s >= 2) & (s < n_sp + 2))
        def _():
            p = s - 2
            a_y(p).wait_recv()
            qs[p % SLOTS, y, :, 0] = (qs[p % SLOTS, y, :, 0].astype(F32) + r2y[p].astype(F32)).astype(BF16)
            t = qs[p % SLOTS, :, x, 1].astype(F32)
            for j in range(1, X):
                a_x(p, j).wait_recv()
                t = t + r2x[p, j - 1].astype(F32)
            qs[p % SLOTS, :, x, 1] = t.astype(BF16)
            b_y(p).start()
            for j in range(1, X):
                b_x(p, j).start()

        @pl.when(s < n_sp)
        def _():
            to_sib(s).wait_recv()
            own = ret[: 2 * X * mine, :cols].reshape(2, X, 2, hm, cols)
            qs[s % SLOTS] = (own.astype(BF16).astype(F32) + r1[s].astype(F32)).astype(BF16)
            a_y(s).start()
            for j in range(1, X):
                a_x(s, j).start()

        @pl.when(s >= 4)
        def _():
            p = s - 4
            u = block_of(p)
            at = pl.ds(pl.multiple_of(u * cols, cols), cols)
            t = upd[:hm, at].astype(F32) + qs[p % SLOTS, y, x, 0].astype(F32)
            for j in range(1, X):
                b_x(p, j).wait_recv()
                t = t + r3x[p, j - 1].astype(F32)
            out[:hm, at] = t.astype(BF16)
            b_y(p).wait_recv()
            t = upd[hm:, at].astype(F32) + qs[p % SLOTS, y, x, 1].astype(F32) + r3y[p].astype(F32)
            out[hm:, at] = t.astype(BF16)
            a_y(p).wait_send()
            b_y(p).wait_send()
            for j in range(1, X):
                a_x(p, j).wait_send()
                b_x(p, j).wait_send()

        return carry

    lax.fori_loop(0, n_sp + 4, step, 0)
    for s in (n_sp - 2, n_sp - 1):
        to_sib(s).wait_send()
    for cond, end in pending:
        if cond is None:
            end()
        else:
            pl.when(cond)(end)


def body(n_sp, n_tp, resid, queries, keys, values, gates, log_decay, w_out, gain, up, down):
    X, Z = n_tp // 2, n_sp // 2
    rows, heads = queries.shape[0], log_decay.shape[0]
    mine, d = resid.shape
    half, cols, part = up.shape[1] // 2, down.shape[1], up.shape[0]
    freq = 10000.0 ** (-np.arange(0, DK, 2, dtype=np.float64) / DK)
    low = np.arange(BLOCK)[:, None] * freq[None, :]
    high = (BLOCK * np.arange(rows * n_sp // BLOCK))[:, None] * freq[None, :]
    tables = [jnp.asarray(f(a), F32) for a in (low, high) for f in (np.cos, np.sin)]
    vm, anym = pl.BlockSpec(memory_space=pltpu.VMEM), pl.BlockSpec(memory_space=pl.ANY)
    dma = pltpu.SemaphoreType.DMA
    V = pltpu.VMEM
    hd, hv = heads * DK, heads * DV
    sq = (DK, DV // 2)
    scratch = [
        V((rows, hd), BF16), V((rows, hd), BF16), V((rows, hv), BF16), V((rows, hv), BF16),
        V((2 * X * mine, 2 * half), BF16), V((mine, d), BF16),
        V((heads, rows, DK), BF16), V((rows, DK), BF16),
        V((2, heads, *sq), F32), V((2, heads, *sq), BF16), V((DK, DV), F32),
        V((heads, *sq), BF16), V((8, DV // 2), F32), V((8, DV // 2), F32),
        V((heads, *sq), BF16), V((heads, *sq), BF16), V((heads, *sq), BF16), V((2, heads, *sq), BF16),
        V((rows, hv), F32),
        V((X, mine, d), BF16), V((X, mine, d), BF16), V((X - 1, mine, d), BF16), V((X - 1, mine, d), BF16),
        V((mine, d), F32), V((mine, d), BF16),
        V((2, 2, X, mine, d), BF16), V((n_sp, part, half), BF16), V((n_sp, half, cols), BF16),
        V((2, 2, X, 2, mine // 2, cols), BF16),
        V((SLOTS, 2, X, 2, mine // 2, cols), BF16), V((n_sp, 2, X, 2, mine // 2, cols), BF16),
        V((n_sp, X, mine // 2, cols), BF16), V((n_sp, X - 1, 2, mine // 2, cols), BF16),
        V((n_sp, mine // 2, cols), BF16), V((n_sp, X - 1, mine // 2, cols), BF16),
        dma((7 + 2 * X * mine // hv,)), dma((2, n_sp, 2)), dma((2, n_sp)), dma((2,)), dma((2,)),
        dma((4, heads)), dma((4, heads)), dma((X, 2)), dma((X, 2)), dma((X, ROWS)), dma((X, ROWS)),
        dma((4, X, ROWS)), dma((X, ROWS)), dma((X, ROWS)), dma((2, X, ROWS)),
        dma((4 + 2 * X, n_sp)), dma((4 + 2 * X, n_sp)),
    ]
    return pl.pallas_call(
        functools.partial(kernel, n_sp, n_tp),
        in_specs=[anym] * 5 + [vm, anym, vm, anym, anym] + [vm] * 4,
        out_specs=vm,
        out_shape=jax.ShapeDtypeStruct((mine, d), BF16),
        scratch_shapes=scratch,
        compiler_params=pltpu.CompilerParams(
            collective_id=0, has_side_effects=True, vmem_limit_bytes=67043328
        ),
        name="layer",
    )(resid, queries, keys, values, gates, log_decay, w_out, gain.reshape(1, d), up, down, *tables)


def solution(mesh):
    placed = (
        P(("sp", "tp"), None),
        P("sp", "tp"),
        P("sp", "tp"),
        P("sp", "tp"),
        P("sp", "tp"),
        P("tp", "sp"),
        P("tp", None),
        P(),
        P("sp", "tp"),
        P("tp", "sp"),
    )
    return jax.shard_map(
        functools.partial(body, mesh.shape["sp"], mesh.shape["tp"]),
        mesh=mesh,
        in_specs=placed,
        out_specs=P(("sp", "tp"), None),
        check_vma=False,
    )
```

```python
import functools

import jax
import jax.numpy as jnp
import numpy as np
from jax import lax
from jax.experimental import pallas as pl
from jax.experimental.pallas import tpu as pltpu
from jax.sharding import PartitionSpec as P

DK = 256
DV = 512
BLOCK = 128
SPAN = 256
ROWS = 4
SLOTS = 5
EPS = 1e-06
F32 = jnp.float32
BF16 = jnp.bfloat16
MESH = pl.DeviceIdType.MESH


def dot(a, b):
    return jnp.dot(a, b, preferred_element_type=F32)


def cumulative(row):
    n = row.shape[1]
    i = lax.broadcasted_iota(jnp.int32, (n, n), 0)
    j = lax.broadcasted_iota(jnp.int32, (n, n), 1)
    col = jnp.sum(jnp.where(i == j, row, 0.0), axis=1, keepdims=True)
    cum_col = jnp.sum(jnp.where(j <= i, row, 0.0), axis=1, keepdims=True)
    cum_row = jnp.sum(jnp.where(i <= j, col, 0.0), axis=0, keepdims=True)
    total = jnp.sum(row, axis=1, keepdims=True)
    return i, j, cum_col, cum_row, total


def kernel(
    n_sp, n_tp,
    resid_h, q_h, k_h, v_h, g_h, ld_h, wo_h, gain, up_h, dn_h, low_h, high_h,
    out_h,
    ld, low, high, out, q_v, k_v, v_v, g_v, wide, res_v, kr, kd, stf, sth, strun, yst, tot, ytot, crecv, csend, esend, inc, ret,
    pp, pr, psum, xr, acc, upd, x_all, up_all, dn_all, pd, qs, r1, r2y, r2x, r3y, r3x,
    lsem, wsend, wrecv, wlast, wysend, wyrecv, ssend, srecv, psend, precv, xsend, xrecv,
    asend, arx, ary, ard, dsem, drecv, qsem, qrecv, osem,
):
    Z, X = n_sp // 2, n_tp // 2
    sp, tp = lax.axis_index("sp"), lax.axis_index("tp")
    z, y = sp // 2, sp % 2
    x, c = tp // 2, tp % 2
    rows = k_v.shape[0]
    heads = kr.shape[0]
    mine = res_v.shape[0]
    d = res_v.shape[1]
    half = up_all.shape[2]
    cols = dn_all.shape[2]
    nblk, nspan = rows // BLOCK, rows // SPAN
    rc = mine // ROWS
    has_up, has_dn = z < Z - 1, z > 0
    halves = cols % 256 == 0 and Z > 2
    cw = cols // 2

    def rcopy(src, dst, ss, rs, dev):
        return pltpu.make_async_remote_copy(src, dst, ss, rs, device_id=dev, device_id_type=MESH)

    to_zp, to_zm = {"sp": sp + 2}, {"sp": sp - 2}
    to_y = {"sp": z * 2 + (1 - y)}
    to_c = {"tp": x * 2 + (1 - c)}

    def xat(j):
        return lax.rem(x + j + X, X)

    def to_x(j):
        return {"tp": xat(j) * 2 + c}

    pending = []

    def send(src, dst, ss, rs, dev, cond=None, track=True):
        def go():
            rcopy(src, dst, ss, rs, dev).start()

        if cond is None:
            go()
        else:
            pl.when(cond)(go)
        if track:
            sent(src, ss, cond)

    def sent(ref, ss, cond=None):
        pending.append((cond, lambda: rcopy(ref, ref, ss, ss, to_c).wait_send()))

    def recv(dst, ss, rs):
        rcopy(dst, dst, ss, rs, to_c).wait_recv()

    loads = [
        (k_h, k_v), (v_h, v_v), (q_h, q_v), (g_h, g_v), (resid_h, res_v),
        (up_h.at[:, pl.ds(pl.multiple_of(y * half, half), half)], up_all.at[sp]),
        (dn_h.at[pl.ds(pl.multiple_of(y * half, half), half), :], dn_all.at[sp]),
    ]
    hv = v_v.shape[1]
    stack = wide.shape[0] // hv
    wc = d // stack
    loads += [(ld_h, ld), (low_h, low), (high_h, high)]
    loads += [(wo_h.at[:, pl.ds(i * wc, wc)], wide.at[pl.ds(i * hv, hv)]) for i in range(stack)]

    def load(i):
        return pltpu.make_async_copy(loads[i][0], loads[i][1], lsem.at[i])

    for i in (7, 8, 9, 0, 1):
        load(i).start()

    barrier = pltpu.get_barrier_semaphore()
    greet = [(to_y, None), (to_c, None)] + [(to_x(j), None) for j in range(1, X)]
    greet += [(to_zp, has_up), (to_zm, has_dn)]
    for dev, cond in greet:
        def hello(dev=dev):
            pl.semaphore_signal(barrier, 1, device_id=dev, device_id_type=MESH)
        if cond is None:
            hello()
        else:
            pl.when(cond)(hello)
    pl.semaphore_wait(barrier, X + 1 + jnp.where(has_up, 1, 0) + jnp.where(has_dn, 1, 0))

    h_up = up_h.at[:, pl.ds(pl.multiple_of(y * half, half), half)]
    h_dn = dn_h.at[pl.ds(pl.multiple_of(y * half, half), half), :]
    o_up = up_h.at[:, pl.ds(pl.multiple_of((1 - y) * half, half), half)]
    o_dn = dn_h.at[pl.ds(pl.multiple_of((1 - y) * half, half), half), :]
    alls = (up_all, dn_all)

    def zsem(w, piece, way):
        return wsend.at[w, n_sp + piece % 2 if way else piece]

    def zsend(w, piece, src, way):
        dev, cond = ((to_zp, has_up), (to_zm, has_dn))[way]
        send(src, alls[w].at[piece], zsem(w, piece, way), wrecv.at[w, piece], dev, cond)

    late = z >= 2
    early = jnp.logical_not(late)
    for way in range(2):
        zsend(0, sp, h_up, way)
    zsend(1, sp, h_dn, 1)

    def own_dn():
        return rcopy(h_dn, dn_all.at[sp], zsem(1, sp, 0), wrecv.at[1, sp], to_zp)

    @pl.when(late & has_up)
    def _():
        own_dn().start()

    pending.append((has_up, lambda: own_dn().wait_send()))
    hr = up_h.shape[0] // 2
    other = z * 2 + (1 - y)

    def ysend(w, src):
        send(src, alls[w].at[sp], wysend.at[w], wyrecv.at[w], to_y)

    def recv_y(w):
        recv(alls[w].at[other], wysend.at[w], wyrecv.at[w])

    def relays(w, k, yy):
        parts = []
        low, high = (z - k) * 2 + yy, (z + k) * 2 + yy
        for piece, way, cond in ((low, 0, (z >= k) & has_up), (high, 1, (z + k < Z) & has_dn)):
            ref, sem, dev = alls[w].at[piece], wsend.at[w, piece], (to_zp, to_zm)[way]

            def go(ref=ref, sem=sem, dev=dev, piece=piece):
                recv(ref, sem, wrecv.at[w, piece])
                if halves and (w, k, yy) == (1, Z - 2, 1):
                    for h in range(2):
                        part = ref.at[:, pl.ds(h * cw, cw)]
                        rcopy(part, part, sem, wlast.at[h], dev).start()
                else:
                    rcopy(ref, ref, sem, wrecv.at[w, piece], dev).start()

            sent(ref, sem, cond)
            parts.append((cond, go))
        return parts

    def fwd(w, k, yy):
        if k <= Z - 2:
            for cond, go in relays(w, k, yy):
                pl.when(cond)(go)

    def settle(w, piece):
        plane = piece // 2
        cond = ((plane < z) & jnp.logical_not(has_up)) | ((plane > z) & jnp.logical_not(has_dn))

        @pl.when(cond)
        def _():
            recv(alls[w].at[piece], wsend.at[w, piece], wrecv.at[w, piece])

    def angles(b):
        at = sp * nblk + b
        hc, hs = high[0, pl.ds(at, 1), :], high[1, pl.ds(at, 1), :]
        lc, ls = low[0], low[1]
        return hc * lc - hs * ls, hs * lc + hc * ls

    def rotated(blk, co, si):
        a, b = blk[:, : DK // 2].astype(F32), blk[:, DK // 2 :].astype(F32)
        return jnp.concatenate([a * co - b * si, a * si + b * co], axis=1)

    tot[...] = jnp.zeros_like(tot)
    for i in (2, 3, *range(10, len(loads)), 4, 5, 6):
        load(i).start()
    for i in (7, 8, 9, 0):
        load(i).wait()
    for h in range(heads):
        def state_block(t, after, h=h):
            b = nblk - 1 - t
            at = pl.ds(pl.multiple_of(b * BLOCK, BLOCK), BLOCK)
            row = ld[h : h + 1, pl.ds(pl.multiple_of(b * BLOCK, BLOCK), BLOCK)]
            i, j, cum_col, _, total = cumulative(row)
            co, si = angles(b)
            key = (rotated(k_v[at, h * DK : (h + 1) * DK], co, si) * DK ** (-0.5)).astype(BF16)
            kr[h, at, :] = key
            kd[at, :] = (key.astype(F32) * jnp.exp(total - cum_col + after)).astype(BF16)
            return after + total

        whole = lax.fori_loop(0, nblk, state_block, jnp.zeros((1, 1), F32))
        tot[h : h + 1, :] = jnp.broadcast_to(jnp.exp(whole), (1, tot.shape[1]))
        if h == 0:
            load(1).wait()
        s = lax.dot_general(kd[...], v_v[:, h * DV : (h + 1) * DV], (((0,), (0,)), ((), ())), preferred_element_type=F32)
        for p in range(2):
            part = s[:, p * DV // 2 : (p + 1) * DV // 2]
            stf[p, h] = part
            sth[p, h] = part.astype(BF16)
        send(sth.at[1 - y, h], yst.at[h], ssend.at[0], srecv.at[0], to_y, track=False)
    sent(sth.at[1 - y], ssend.at[0])
    send(tot, ytot, ssend.at[3], srecv.at[2], to_y)
    ysend(0, o_up)
    ysend(1, o_dn)

    load(2).wait()

    def local(h):
        strun[...] = jnp.zeros_like(strun)

        def span(t, before):
            at = pl.ds(pl.multiple_of(t * SPAN, SPAN), SPAN)
            row = ld[h : h + 1, pl.ds(pl.multiple_of(t * SPAN, SPAN), SPAN)]
            i, j, cum_col, cum_row, total = cumulative(row)
            parts = []
            for u in range(SPAN // BLOCK):
                co, si = angles(t * (SPAN // BLOCK) + u)
                qat = pl.ds(pl.multiple_of(t * SPAN + u * BLOCK, BLOCK), BLOCK)
                parts.append(rotated(q_v[qat, h * DK : (h + 1) * DK], co, si))
            query = jnp.concatenate(parts, axis=0).astype(BF16)
            key = kr[h, at, :]
            factor = jnp.where(i >= j, jnp.exp(jnp.minimum(cum_col - cum_row, 0.0)), 0.0)
            scores = lax.dot_general(query, key, (((1,), (1,)), ((), ())), preferred_element_type=F32)
            weights = (scores * factor).astype(BF16)
            q32 = query.astype(F32)
            val = v_v[at, h * DV : (h + 1) * DV]
            ret[at, h * DV : (h + 1) * DV] = dot(weights, val) + dot((q32 * jnp.exp(cum_col)).astype(BF16), strun[...].astype(BF16))
            q_v[at, h * DK : (h + 1) * DK] = (q32 * jnp.exp(cum_col + before)).astype(BF16)
            kdec = (key.astype(F32) * jnp.exp(total - cum_col)).astype(BF16)
            strun[...] = jnp.exp(total) * strun[...] + lax.dot_general(
                kdec, val, (((0,), (0,)), ((), ())), preferred_element_type=F32
            )
            return before + total

        lax.fori_loop(0, nspan, span, jnp.zeros((1, 1), F32))

    local(0)

    first = y == 0
    recv(ytot, ssend.at[3], srecv.at[2])
    recv(yst, ssend.at[0], srecv.at[0])

    def decays(h):
        own, oth = tot[h : h + 1, : DV // 2], ytot[h : h + 1, : DV // 2]
        return jnp.where(first, own, oth), jnp.where(first, oth, own)

    @pl.when(jnp.logical_not(has_dn))
    def _():
        crecv[...] = jnp.zeros_like(crecv)

    def s_pair(h):
        own, oth = stf[y, h], yst[h].astype(F32)
        return jnp.where(first, own, oth), jnp.where(first, oth, own)

    def chain(h):
        d0, d1 = decays(h)
        s0, s1 = s_pair(h)
        csend[h] = (d0 * d1 * crecv[h].astype(F32) + (d1 * s0 + s1)).astype(BF16)

    def chain_send(h):
        rcopy(csend.at[h], crecv.at[h], ssend.at[1], srecv.at[3 + h], to_zp).start()

    @pl.when(jnp.logical_not(has_dn))
    def _():
        for h in range(heads):
            chain(h)
            chain_send(h)
        own_dn().start()

    for h in range(1, heads):
        local(h)

    def part_up(part):
        ref = up_all.at[other, pl.ds(part * hr, hr)]
        rcopy(ref, ref, zsem(0, other, 0), wrecv.at[0, other], to_zp).start()

    @pl.when(late)
    def _():
        recv_y(0)
        pl.when(has_up)(lambda: part_up(0))

    @pl.when(has_dn)
    def _():
        for h in range(heads):
            recv(crecv.at[h], ssend.at[1], srecv.at[3 + h])

            @pl.when(has_up)
            def _():
                chain(h)
                chain_send(h)

        @pl.when(early & has_up)
        def _():
            own_dn().start()

    def chain_end():
        rcopy(csend, crecv, ssend.at[1], srecv.at[0], to_zp).wait_send()
        rcopy(up_all.at[other], up_all.at[other], zsem(0, other, 0), wrecv.at[0, other], to_zp).wait_send()

    pending.append((has_up, chain_end))
    for h in range(heads):
        d0, _ = decays(h)
        s0, _ = s_pair(h)
        got = crecv[h].astype(F32)
        later = (d0 * got + s0).astype(BF16)
        inc[y, h] = jnp.where(first, crecv[h], later)
        esend[h] = jnp.where(first, later, crecv[h])
        send(esend.at[h], inc.at[y, h], ssend.at[2], srecv.at[1], to_y, track=False)
    @pl.when(early)
    def _():
        recv_y(0)
        pl.when(has_up)(lambda: part_up(0))

    pl.when(has_up)(lambda: part_up(1))
    zsend(0, other, up_all.at[other], 1)
    fwd(0, 1, y)
    load(3).wait()
    for i in range(stack):
        load(10 + i).wait()
    sent(esend, ssend.at[2])
    recv(inc.at[1 - y], ssend.at[2], srecv.at[1])

    ph = mine // 2
    fr = min(128, ph)

    def finish(base):

        def part(t, carry):
            at = pl.ds(pl.multiple_of(base + t * fr, fr), fr)
            for h in range(heads):
                qd = q_v[at, h * DK : (h + 1) * DK]
                r = ret[at, h * DV : (h + 1) * DV] + jnp.concatenate([dot(qd, inc[0, h]), dot(qd, inc[1, h])], axis=1)
                normed = r * lax.rsqrt(jnp.mean(r * r, axis=1, keepdims=True) + EPS)
                g = g_v[at, h * DV : (h + 1) * DV].astype(F32)
                g_v[at, h * DV : (h + 1) * DV] = (g / (1.0 + jnp.exp(-g)) * normed).astype(BF16)
            return carry

        lax.fori_loop(0, ph // fr, part, 0)

    pt = min(512, wc)

    def project(base, put):
        rows_at = pl.ds(pl.multiple_of(base, ph), ph)
        for i in range(stack):
            def part(t, carry, i=i):
                at = pl.ds(pl.multiple_of(t * pt, pt), pt)
                to = pl.ds(pl.multiple_of(i * wc + t * pt, pt), pt)
                put(to, dot(g_v[rows_at, :], wide[i * hv : (i + 1) * hv, at]))
                return carry

            lax.fori_loop(0, wc // pt, part, 0)

    def for_sibling(j, p):
        base = (xat(j) * 2 + (1 - c)) * mine + p * ph
        finish(base)
        mid = pl.ds(p * ph, ph)

        def put(at, val):
            pp[j, mid, at] = val.astype(BF16)

        project(base, put)
        send(pp.at[j, mid], pr.at[j, mid], psend.at[j], precv.at[j, p], to_c, track=False)

    def for_mine(j, p):
        base = (xat(j) * 2 + c) * mine + p * ph
        finish(base)
        mid = pl.ds(p * ph, ph)

        def put(at, val):
            acc[mid, at] = val.astype(BF16).astype(F32)

        project(base, put)
        recv(pr.at[j, mid], psend.at[j], precv.at[j, p])
        if j:
            for r in range(p * ROWS // 2, (p + 1) * ROWS // 2):
                at = pl.ds(r * rc, rc)
                psum[j - 1, at, :] = (acc[at, :] + pr[j, at, :].astype(F32)).astype(BF16)
                send(psum.at[j - 1, at], xr.at[j - 1, at], xsend.at[j - 1], xrecv.at[j - 1, r], to_x(j), track=False)

    for j in range(1, X):
        for p in range(2):
            for_sibling(j, p)
            for_mine(j, p)
    fwd(0, 1, 1 - y)
    for p in range(2):
        for_sibling(0, p)
        for_mine(0, p)
    recv_y(1)
    for way in range(2):
        zsend(1, other, dn_all.at[other], way)
    fwd(0, 2, y)

    for j in range(X):
        sent(pp.at[j], psend.at[j])
        if j:
            sent(psum.at[j - 1], xsend.at[j - 1])

    load(4).wait()
    for r in range(ROWS):
        at = pl.ds(r * rc, rc)
        s = acc[at, :] + pr[0, at, :].astype(F32)
        for j in range(1, X):
            recv(xr.at[j - 1, at], xsend.at[j - 1], xrecv.at[j - 1, r])
            s = s + xr[j - 1, at, :].astype(F32)
        u = (res_v[at, :].astype(F32) + s).astype(BF16)
        upd[at, :] = u
        u = u.astype(F32)
        u = u * lax.rsqrt(jnp.mean(u * u, axis=1, keepdims=True) + EPS)
        x_all[c, y, x, at, :] = (u * gain[...].astype(F32).reshape(1, d)).astype(BF16)
        own = x_all.at[c, y, x, at]
        send(own, own, asend.at[0, 0], ary.at[0, r], to_y, track=False)
        for j in range(1, X):
            send(own, own, asend.at[1, j], arx.at[j, r], to_x(j), track=False)
        send(own, own, asend.at[2, 0], ard.at[0, 0], to_c, track=False)

    load(5).wait()
    for k in range(1, Z - 1):
        if k == 1:
            continue
        fwd(0, k, 1 - y)
        if k > 2:
            fwd(0, k, y)

    ht = min(512, half)

    def hid_rows(yy, xx):
        return pl.ds(pl.multiple_of((yy * X + xx) * mine, mine), mine)

    def hid_of(cc):
        return pl.ds(pl.multiple_of(cc * half, half), half)

    def hidden(yy, xx):
        def part(t, carry):
            at = pl.ds(pl.multiple_of(t * ht, ht), ht)
            w = up_all[:, :, at].reshape(d, ht)
            for cc in range(2):
                pre = jnp.maximum(dot(x_all[cc, yy, xx], w), 0.0)
                col = pl.ds(pl.multiple_of(cc * half + t * ht, ht), ht)
                wide[hid_rows(yy, xx), col] = (pre * pre).astype(BF16)
            return carry

        lax.fori_loop(0, half // ht, part, 0)

    for i in range(X):
        for kind, yy in ((0, y), (2, y), (3, 1 - y)):
            sent(x_all.at[c, yy, xat(-i)], asend.at[kind, i])
        if i:
            sent(x_all.at[c, y, x], asend.at[1, i])

    def from_sibling(yrel, i):
        recv(x_all.at[1 - c, (1 - y) if yrel else y, xat(-i)], asend.at[2, 0], ard.at[yrel, i])

    def pass_on(yrel, i, r):
        at = pl.ds(r * rc, rc)
        ref = x_all.at[c, (1 - y) if yrel else y, xat(-i), at]
        if yrel:
            recv(ref, asend.at[0, 0], ary.at[i, r])
        else:
            recv(ref, asend.at[1, i], arx.at[i, r])
            send(ref, ref, asend.at[0, i], ary.at[i, r], to_y, track=False)
        send(ref, ref, asend.at[2 + yrel, i], ard.at[yrel, i], to_c, track=False)

    for r in range(ROWS):
        pass_on(1, 0, r)
    for r in range(ROWS):
        for j in range(1, X):
            pass_on(0, j, r)
        if r == 1:
            fwd(1, 1, 0)
    fwd(1, 1, 1)
    for k in range(n_sp):
        settle(0, k)
    from_sibling(0, 0)
    hidden(y, x)
    from_sibling(1, 0)
    hidden(1 - y, x)
    for j in range(1, X):
        for r in range(ROWS):
            pass_on(1, j, r)
        from_sibling(0, j)
        hidden(y, xat(-j))
    for j in range(1, X):
        from_sibling(1, j)
        hidden(1 - y, xat(-j))

    load(6).wait()
    m = jnp.minimum(z, Z - 1 - z)
    hm = mine // 2

    def block_of(s):
        i = s // 2
        near = jnp.where(i % 2 == 1, z - (i + 1) // 2, z + i // 2)
        far = jnp.where(z <= Z - 1 - z, i, Z - 1 - i)
        return jnp.where(i <= 2 * m, near, far) * 2 + s % 2

    units = n_sp - 1 if halves else n_sp
    total = units + 2 if halves else units
    na, nb = 3 * X - 2, X

    class Unit:
        def __init__(self, t, part=None):
            self.t, self.u = t, (t if part is None else n_sp - 1)
            self.w = cols if part is None else cw
            self.c0 = 0 if part is None else part * cw
            self.block = block_of(self.u)

        def trim(self, ref, start):
            return ref if self.w == cols else ref.at[..., pl.ds(start, self.w)]

        def bulk(self, n, ss, rs):
            ref = wide.at[pl.ds(0, n * hm), pl.ds(0, self.w)]
            return rcopy(ref, ref, ss, rs, to_c)

        def to_sib(self):
            t = self.t
            return rcopy(self.trim(pd.at[t % 2], 0), self.trim(r1.at[self.u], self.c0), dsem.at[t % 2], drecv.at[t], to_c)

        def copies(self, stage):
            q, t, u = qs.at[self.t % SLOTS], self.t, self.u
            if stage == 0:
                pairs = [(q.at[1 - y, :, 0], r2y.at[u], to_y)]
                pairs += [(q.at[:, xat(j), 1], r2x.at[u, j - 1], to_x(j)) for j in range(1, X)]
            else:
                pairs = [(q.at[1 - y, x, 1], r3y.at[u], to_y)]
                pairs += [(q.at[y, xat(j), 0], r3x.at[u, j - 1], to_x(j)) for j in range(1, X)]
            for src, dst, dev in pairs:
                rcopy(self.trim(src, 0), self.trim(dst, self.c0), qsem.at[stage, t % SLOTS], qrecv.at[stage, t], dev).start()

        def wait_sib(self):
            ref = self.trim(pd.at[self.t % 2], 0)
            rcopy(ref, ref, dsem.at[self.t % 2], drecv.at[self.t], to_c).wait_send()

        def compute(self, before):
            if self.w == cols:
                settle(1, self.block)
            else:
                @pl.when(jnp.logical_not(has_up & has_dn))
                def _():
                    ref = dn_all.at[self.block, :, pl.ds(self.c0, cw)]
                    recv(ref, wsend.at[1, 0], wlast.at[self.c0 // cw])
            if before is not None:
                before()
            w = dn_all[self.block, :, self.c0 : self.c0 + self.w]
            pd[self.t % 2, :, :, :, :, : self.w] = dot(wide[:, hid_of(1 - c)], w).astype(BF16).reshape(2, X, 2, hm, self.w)
            self.to_sib().start()
            ret[: 2 * X * mine, : self.w] = dot(wide[:, hid_of(c)], w)

        def first(self):
            k, at = self.t % SLOTS, slice(self.c0, self.c0 + self.w)
            self.to_sib().wait_recv()
            own = ret[: 2 * X * mine, : self.w].reshape(2, X, 2, hm, self.w)
            qs[k, :, :, :, :, : self.w] = (own.astype(BF16).astype(F32) + r1[self.u, :, :, :, :, at].astype(F32)).astype(BF16)
            self.copies(0)

        def second(self):
            k, at, w = self.t % SLOTS, slice(self.c0, self.c0 + self.w), self.w
            self.bulk(na, qsem.at[0, 0], qrecv.at[0, self.t]).wait_recv()
            qs[k, y, :, 0, :, :w] = (qs[k, y, :, 0, :, :w].astype(F32) + r2y[self.u, :, :, at].astype(F32)).astype(BF16)
            s = qs[k, :, x, 1, :, :w].astype(F32)
            for j in range(1, X):
                s = s + r2x[self.u, j - 1, :, :, at].astype(F32)
            qs[k, :, x, 1, :, :w] = s.astype(BF16)
            self.copies(1)

        def put(self):
            at = pl.ds(pl.multiple_of(self.block * cols + self.c0, 128), self.w)
            return pltpu.make_async_copy(self.trim(out.at[self.t % 4], 0), out_h.at[:, at], osem.at[self.t % 4])

        def final(self):
            k, at, w = self.t % SLOTS, slice(self.c0, self.c0 + self.w), self.w
            o = self.t % 4
            col = pl.ds(pl.multiple_of(self.block * cols + self.c0, 128), w)
            self.bulk(nb, qsem.at[1, 0], qrecv.at[1, self.t]).wait_recv()
            s = upd[:hm, col].astype(F32) + qs[k, y, x, 0, :, :w].astype(F32)
            for j in range(1, X):
                s = s + r3x[self.u, j - 1, :, at].astype(F32)
            out[o, :hm, :w] = s.astype(BF16)
            s = upd[hm:, col].astype(F32) + qs[k, y, x, 1, :, :w].astype(F32) + r3y[self.u, :, at].astype(F32)
            out[o, hm:, :w] = s.astype(BF16)
            self.put().start()
            self.bulk(na, qsem.at[0, k], qrecv.at[0, 0]).wait_send()
            self.bulk(nb, qsem.at[1, k], qrecv.at[1, 0]).wait_send()

    last = [(2 * (k - 2 + yy), relays(1, k, yy)) for k in range(2, Z - 1) for yy in range(2)]

    def step(s, carry):
        for at, parts in last:
            for cond, go in parts:
                pl.when(cond & (s == at))(go)
        Unit(s).compute(lambda: pl.when(s >= 2)(lambda: Unit(s - 2).wait_sib()))

        @pl.when(s >= 2)
        def _():
            Unit(s - 2).second()

        Unit(s).first()

        @pl.when(s >= 4)
        def _():
            pl.when(s >= 8)(lambda: Unit(s - 8).put().wait())
            Unit(s - 4).final()

        return carry

    lax.fori_loop(0, units, step, 0)
    tail = [Unit(t) for t in range(units)]
    if halves:
        tail += [Unit(units + p, p) for p in range(2)]
        for t in range(units, total):
            tail[t].compute(tail[t - 2].wait_sib)
            tail[t - 2].second()
            tail[t].first()
            if t >= 8:
                tail[t - 8].put().wait()
            tail[t - 4].final()
    tail[total - 2].second()
    tail[total - 1].second()
    for t in range(total - 4, total):
        if t >= 4:
            tail[t - 4].put().wait()
        tail[t].final()
    for t in range(total - 4, total):
        tail[t].put().wait()
    for t in range(total - 2, total):
        tail[t].wait_sib()
    for cond, end in pending:
        if cond is None:
            end()
        else:
            pl.when(cond)(end)


def body(n_sp, n_tp, resid, queries, keys, values, gates, log_decay, w_out, gain, up, down):
    X, Z = n_tp // 2, n_sp // 2
    rows, heads = queries.shape[0], log_decay.shape[0]
    mine, d = resid.shape
    half, cols, part = up.shape[1] // 2, down.shape[1], up.shape[0]
    freq = 10000.0 ** (-np.arange(0, DK, 2, dtype=np.float64) / DK)
    near = np.arange(BLOCK)[:, None] * freq[None, :]
    far = (BLOCK * np.arange(rows * n_sp // BLOCK))[:, None] * freq[None, :]
    tables = [jnp.asarray(np.stack([np.cos(a), np.sin(a)]), F32) for a in (near, far)]
    vm, anym = pl.BlockSpec(memory_space=pltpu.VMEM), pl.BlockSpec(memory_space=pl.ANY)
    dma = pltpu.SemaphoreType.DMA
    V = pltpu.VMEM
    hd, hv = heads * DK, heads * DV
    sq = (DK, DV // 2)
    scratch = [
        V((heads, rows), F32), *[V(t.shape, F32) for t in tables], V((4, mine, cols), BF16),
        V((rows, hd), BF16), V((rows, hd), BF16), V((rows, hv), BF16), V((rows, hv), BF16),
        V((2 * X * mine, 2 * half), BF16), V((mine, d), BF16),
        V((heads, rows, DK), BF16), V((rows, DK), BF16),
        V((2, heads, *sq), F32), V((2, heads, *sq), BF16), V((DK, DV), F32),
        V((heads, *sq), BF16), V((8, DV // 2), F32), V((8, DV // 2), F32),
        V((heads, *sq), BF16), V((heads, *sq), BF16), V((heads, *sq), BF16), V((2, heads, *sq), BF16),
        V((rows, hv), F32),
        V((X, mine, d), BF16), V((X, mine, d), BF16), V((X - 1, mine, d), BF16), V((X - 1, mine, d), BF16),
        V((mine, d), F32), V((mine, d), BF16),
        V((2, 2, X, mine, d), BF16), V((n_sp, part, half), BF16), V((n_sp, half, cols), BF16),
        V((2, 2, X, 2, mine // 2, cols), BF16),
        V((SLOTS, 2, X, 2, mine // 2, cols), BF16), V((n_sp, 2, X, 2, mine // 2, cols), BF16),
        V((n_sp, X, mine // 2, cols), BF16), V((n_sp, X - 1, 2, mine // 2, cols), BF16),
        V((n_sp, mine // 2, cols), BF16), V((n_sp, X - 1, mine // 2, cols), BF16),
        dma((10 + 2 * X * mine // hv,)), dma((2, n_sp + 2)), dma((2, n_sp)), dma((2,)), dma((2,)), dma((2,)),
        dma((4,)), dma((3 + heads,)), dma((X,)), dma((X, 2)), dma((X - 1,)), dma((X - 1, ROWS)),
        dma((4, X)), dma((X, ROWS)), dma((X, ROWS)), dma((2, X)),
        dma((2,)), dma((n_sp + 1,)), dma((2, SLOTS)), dma((2, n_sp + 1)), dma((4,)),
    ]
    return pl.pallas_call(
        functools.partial(kernel, n_sp, n_tp),
        in_specs=[anym] * 7 + [vm] + [anym] * 4,
        out_specs=anym,
        out_shape=jax.ShapeDtypeStruct((mine, d), BF16),
        scratch_shapes=scratch,
        compiler_params=pltpu.CompilerParams(
            collective_id=0, has_side_effects=True, vmem_limit_bytes=67043328
        ),
        name="layer",
    )(resid, queries, keys, values, gates, log_decay, w_out, gain, up, down, *tables)


def solution(mesh):
    placed = (
        P(("sp", "tp"), None),
        P("sp", "tp"),
        P("sp", "tp"),
        P("sp", "tp"),
        P("sp", "tp"),
        P("tp", "sp"),
        P("tp", None),
        P(),
        P("sp", "tp"),
        P("tp", "sp"),
    )
    return jax.shard_map(
        functools.partial(body, mesh.shape["sp"], mesh.shape["tp"]),
        mesh=mesh,
        in_specs=placed,
        out_specs=P(("sp", "tp"), None),
        check_vma=False,
    )
```

```python
import functools

import jax
import jax.numpy as jnp
import numpy as np
from jax import lax
from jax.experimental import pallas as pl
from jax.experimental.pallas import tpu as pltpu
from jax.sharding import PartitionSpec as P

DK = 256
DV = 512
BLOCK = 128
SPAN = 256
ROWS = 4
SLOTS = 5
EPS = 1e-06
F32 = jnp.float32
BF16 = jnp.bfloat16
MESH = pl.DeviceIdType.MESH


def dot(a, b):
    return jnp.dot(a, b, preferred_element_type=F32)


def cumulative(row):
    n = row.shape[1]
    i = lax.broadcasted_iota(jnp.int32, (n, n), 0)
    j = lax.broadcasted_iota(jnp.int32, (n, n), 1)
    col = jnp.sum(jnp.where(i == j, row, 0.0), axis=1, keepdims=True)
    cum_col = jnp.sum(jnp.where(j <= i, row, 0.0), axis=1, keepdims=True)
    cum_row = jnp.sum(jnp.where(i <= j, col, 0.0), axis=0, keepdims=True)
    total = jnp.sum(row, axis=1, keepdims=True)
    return i, j, cum_col, cum_row, total


def kernel(
    n_sp, n_tp,
    resid_h, q_h, k_h, v_h, g_h, ld_h, wo_h, gain, up_h, dn_h, low_h, high_h,
    out_h,
    ld, low, high, out, q_v, k_v, v_v, g_v, wide, res_v, kr, kd, stf, sth, strun, yst, tot, ytot, crecv, csend, esend, inc, ret,
    pp, pr, psum, xr, acc, upd, x_all, up_all, dn_all, pd, qs, r1, r2y, r2x, r3y, r3x, rd,
    lsem, wsend, wrecv, wlast, wysend, wyrecv, ssend, srecv, psend, precv, xsend, xrecv,
    asend, arx, ary, ard, dsem, drecv, qsem, qrecv, osem,
):
    Z, X = n_sp // 2, n_tp // 2
    sp, tp = lax.axis_index("sp"), lax.axis_index("tp")
    z, y = sp // 2, sp % 2
    x, c = tp // 2, tp % 2
    rows = k_v.shape[0]
    heads = kr.shape[0]
    mine = res_v.shape[0]
    d = res_v.shape[1]
    half = up_all.shape[2]
    cols = dn_all.shape[2]
    nblk, nspan = rows // BLOCK, rows // SPAN
    rc = mine // ROWS
    has_up, has_dn = z < Z - 1, z > 0
    halves = cols % 256 == 0 and Z > 2
    cw, ka = cols // 2, half - min(256, half // 2)
    pieces = ((0, half, 0), (0, ka, cw), (ka, half - ka, cw))

    def rcopy(src, dst, ss, rs, dev):
        return pltpu.make_async_remote_copy(src, dst, ss, rs, device_id=dev, device_id_type=MESH)

    to_zp, to_zm = {"sp": sp + 2}, {"sp": sp - 2}
    to_y = {"sp": z * 2 + (1 - y)}
    to_c = {"tp": x * 2 + (1 - c)}

    def xat(j):
        return lax.rem(x + j + X, X)

    def to_x(j):
        return {"tp": xat(j) * 2 + c}

    def to_diag(j):
        return {"sp": z * 2 + (1 - y), "tp": xat(j) * 2 + c}

    pending = []

    def send(src, dst, ss, rs, dev, cond=None, track=True):
        def go():
            rcopy(src, dst, ss, rs, dev).start()

        if cond is None:
            go()
        else:
            pl.when(cond)(go)
        if track:
            sent(src, ss, cond)

    def sent(ref, ss, cond=None):
        pending.append((cond, lambda: rcopy(ref, ref, ss, ss, to_c).wait_send()))

    def recv(dst, ss, rs):
        rcopy(dst, dst, ss, rs, to_c).wait_recv()

    loads = [
        (k_h, k_v), (v_h, v_v), (q_h, q_v), (g_h, g_v), (resid_h, res_v),
        (up_h.at[:, pl.ds(pl.multiple_of(y * half, half), half)], up_all.at[sp]),
        (dn_h.at[pl.ds(pl.multiple_of(y * half, half), half), :], dn_all.at[sp]),
    ]
    hv = v_v.shape[1]
    stack = wide.shape[0] // hv
    wc = d // stack
    loads += [(ld_h, ld), (low_h, low), (high_h, high)]
    loads += [(wo_h.at[:, pl.ds(i * wc, wc)], wide.at[pl.ds(i * hv, hv)]) for i in range(stack)]

    def load(i):
        return pltpu.make_async_copy(loads[i][0], loads[i][1], lsem.at[i])

    for i in (7, 8, 9, 0, 1):
        load(i).start()

    barrier = pltpu.get_barrier_semaphore()
    greet = [(to_y, None), (to_c, None)] + [(to_x(j), None) for j in range(1, X)]
    if halves:
        greet += [(to_diag(j), None) for j in range(1, X)]
    greet += [(to_zp, has_up), (to_zm, has_dn)]
    for dev, cond in greet:
        def hello(dev=dev):
            pl.semaphore_signal(barrier, 1, device_id=dev, device_id_type=MESH)
        if cond is None:
            hello()
        else:
            pl.when(cond)(hello)
    pl.semaphore_wait(barrier, X + 1 + halves * (X - 1) + jnp.where(has_up, 1, 0) + jnp.where(has_dn, 1, 0))

    h_up = up_h.at[:, pl.ds(pl.multiple_of(y * half, half), half)]
    h_dn = dn_h.at[pl.ds(pl.multiple_of(y * half, half), half), :]
    o_up = up_h.at[:, pl.ds(pl.multiple_of((1 - y) * half, half), half)]
    o_dn = dn_h.at[pl.ds(pl.multiple_of((1 - y) * half, half), half), :]
    alls = (up_all, dn_all)

    def zsem(w, piece, way):
        return wsend.at[w, n_sp + piece % 2 if way else piece]

    def zsend(w, piece, src, way):
        dev, cond = ((to_zp, has_up), (to_zm, has_dn))[way]
        send(src, alls[w].at[piece], zsem(w, piece, way), wrecv.at[w, piece], dev, cond)

    late = z >= 2
    early = jnp.logical_not(late)
    for way in range(2):
        zsend(0, sp, h_up, way)
    zsend(1, sp, h_dn, 1)

    def own_dn():
        return rcopy(h_dn, dn_all.at[sp], zsem(1, sp, 0), wrecv.at[1, sp], to_zp)

    @pl.when(late & has_up)
    def _():
        own_dn().start()

    pending.append((has_up, lambda: own_dn().wait_send()))
    hr = up_h.shape[0] // 2
    other = z * 2 + (1 - y)

    def ysend(w, src):
        send(src, alls[w].at[sp], wysend.at[w], wyrecv.at[w], to_y)

    def recv_y(w):
        recv(alls[w].at[other], wysend.at[w], wyrecv.at[w])

    def relays(w, k, yy):
        parts = []
        low, high = (z - k) * 2 + yy, (z + k) * 2 + yy
        for piece, way, cond in ((low, 0, (z >= k) & has_up), (high, 1, (z + k < Z) & has_dn)):
            ref, sem, dev = alls[w].at[piece], wsend.at[w, piece], (to_zp, to_zm)[way]

            def go(ref=ref, sem=sem, dev=dev, piece=piece):
                recv(ref, sem, wrecv.at[w, piece])
                if halves and (w, k, yy) == (1, Z - 2, 1):
                    for h, (r0, nr, c0) in enumerate(pieces):
                        part = ref.at[pl.ds(r0, nr), pl.ds(c0, cw)]
                        rcopy(part, part, sem, wlast.at[h], dev).start()
                else:
                    rcopy(ref, ref, sem, wrecv.at[w, piece], dev).start()

            sent(ref, sem, cond)
            parts.append((cond, go))
        return parts

    def fwd(w, k, yy):
        if k <= Z - 2:
            for cond, go in relays(w, k, yy):
                pl.when(cond)(go)

    def settle(w, piece):
        plane = piece // 2
        cond = ((plane < z) & jnp.logical_not(has_up)) | ((plane > z) & jnp.logical_not(has_dn))

        @pl.when(cond)
        def _():
            recv(alls[w].at[piece], wsend.at[w, piece], wrecv.at[w, piece])

    def angles(b):
        at = sp * nblk + b
        hc, hs = high[0, pl.ds(at, 1), :], high[1, pl.ds(at, 1), :]
        lc, ls = low[0], low[1]
        return hc * lc - hs * ls, hs * lc + hc * ls

    def rotated(blk, co, si):
        a, b = blk[:, : DK // 2].astype(F32), blk[:, DK // 2 :].astype(F32)
        return jnp.concatenate([a * co - b * si, a * si + b * co], axis=1)

    tot[...] = jnp.zeros_like(tot)
    for i in (2, 3, *range(10, len(loads)), 4, 5, 6):
        load(i).start()
    for i in (7, 8, 9, 0):
        load(i).wait()
    for h in range(heads):
        def state_block(t, after, h=h):
            b = nblk - 1 - t
            at = pl.ds(pl.multiple_of(b * BLOCK, BLOCK), BLOCK)
            row = ld[h : h + 1, pl.ds(pl.multiple_of(b * BLOCK, BLOCK), BLOCK)]
            i, j, cum_col, _, total = cumulative(row)
            co, si = angles(b)
            key = (rotated(k_v[at, h * DK : (h + 1) * DK], co, si) * DK ** (-0.5)).astype(BF16)
            kr[h, at, :] = key
            kd[at, :] = (key.astype(F32) * jnp.exp(total - cum_col + after)).astype(BF16)
            return after + total

        whole = lax.fori_loop(0, nblk, state_block, jnp.zeros((1, 1), F32))
        tot[h : h + 1, :] = jnp.broadcast_to(jnp.exp(whole), (1, tot.shape[1]))
        if h == 0:
            load(1).wait()
        s = lax.dot_general(kd[...], v_v[:, h * DV : (h + 1) * DV], (((0,), (0,)), ((), ())), preferred_element_type=F32)
        for p in range(2):
            part = s[:, p * DV // 2 : (p + 1) * DV // 2]
            stf[p, h] = part
            sth[p, h] = part.astype(BF16)
        send(sth.at[1 - y, h], yst.at[h], ssend.at[0], srecv.at[0], to_y, track=False)
    sent(sth.at[1 - y], ssend.at[0])
    send(tot, ytot, ssend.at[3], srecv.at[2], to_y)
    ysend(0, o_up)
    ysend(1, o_dn)

    load(2).wait()

    def local(h):
        strun[...] = jnp.zeros_like(strun)

        def span(t, before):
            at = pl.ds(pl.multiple_of(t * SPAN, SPAN), SPAN)
            row = ld[h : h + 1, pl.ds(pl.multiple_of(t * SPAN, SPAN), SPAN)]
            i, j, cum_col, cum_row, total = cumulative(row)
            parts = []
            for u in range(SPAN // BLOCK):
                co, si = angles(t * (SPAN // BLOCK) + u)
                qat = pl.ds(pl.multiple_of(t * SPAN + u * BLOCK, BLOCK), BLOCK)
                parts.append(rotated(q_v[qat, h * DK : (h + 1) * DK], co, si))
            query = jnp.concatenate(parts, axis=0).astype(BF16)
            key = kr[h, at, :]
            factor = jnp.where(i >= j, jnp.exp(jnp.minimum(cum_col - cum_row, 0.0)), 0.0)
            scores = lax.dot_general(query, key, (((1,), (1,)), ((), ())), preferred_element_type=F32)
            weights = (scores * factor).astype(BF16)
            q32 = query.astype(F32)
            val = v_v[at, h * DV : (h + 1) * DV]
            ret[at, h * DV : (h + 1) * DV] = dot(weights, val) + dot((q32 * jnp.exp(cum_col)).astype(BF16), strun[...].astype(BF16))
            q_v[at, h * DK : (h + 1) * DK] = (q32 * jnp.exp(cum_col + before)).astype(BF16)
            kdec = (key.astype(F32) * jnp.exp(total - cum_col)).astype(BF16)
            strun[...] = jnp.exp(total) * strun[...] + lax.dot_general(
                kdec, val, (((0,), (0,)), ((), ())), preferred_element_type=F32
            )
            return before + total

        lax.fori_loop(0, nspan, span, jnp.zeros((1, 1), F32))

    local(0)

    first = y == 0
    recv(ytot, ssend.at[3], srecv.at[2])
    recv(yst, ssend.at[0], srecv.at[0])

    def decays(h):
        own, oth = tot[h : h + 1, : DV // 2], ytot[h : h + 1, : DV // 2]
        return jnp.where(first, own, oth), jnp.where(first, oth, own)

    @pl.when(jnp.logical_not(has_dn))
    def _():
        crecv[...] = jnp.zeros_like(crecv)

    def s_pair(h):
        own, oth = stf[y, h], yst[h].astype(F32)
        return jnp.where(first, own, oth), jnp.where(first, oth, own)

    def chain(h):
        d0, d1 = decays(h)
        s0, s1 = s_pair(h)
        csend[h] = (d0 * d1 * crecv[h].astype(F32) + (d1 * s0 + s1)).astype(BF16)

    def chain_send(h):
        rcopy(csend.at[h], crecv.at[h], ssend.at[1], srecv.at[3 + h], to_zp).start()

    @pl.when(jnp.logical_not(has_dn))
    def _():
        for h in range(heads):
            chain(h)
            chain_send(h)
        own_dn().start()

    for h in range(1, heads):
        local(h)

    def part_up(part):
        ref = up_all.at[other, pl.ds(part * hr, hr)]
        rcopy(ref, ref, zsem(0, other, 0), wrecv.at[0, other], to_zp).start()

    @pl.when(late)
    def _():
        recv_y(0)
        pl.when(has_up)(lambda: part_up(0))

    @pl.when(has_dn)
    def _():
        for h in range(heads):
            recv(crecv.at[h], ssend.at[1], srecv.at[3 + h])

            @pl.when(has_up)
            def _():
                chain(h)
                chain_send(h)

        @pl.when(early & has_up)
        def _():
            own_dn().start()

    def chain_end():
        rcopy(csend, crecv, ssend.at[1], srecv.at[0], to_zp).wait_send()
        rcopy(up_all.at[other], up_all.at[other], zsem(0, other, 0), wrecv.at[0, other], to_zp).wait_send()

    pending.append((has_up, chain_end))
    for h in range(heads):
        d0, _ = decays(h)
        s0, _ = s_pair(h)
        got = crecv[h].astype(F32)
        later = (d0 * got + s0).astype(BF16)
        inc[y, h] = jnp.where(first, crecv[h], later)
        esend[h] = jnp.where(first, later, crecv[h])
        send(esend.at[h], inc.at[y, h], ssend.at[2], srecv.at[1], to_y, track=False)
    @pl.when(early)
    def _():
        recv_y(0)
        pl.when(has_up)(lambda: part_up(0))

    pl.when(has_up)(lambda: part_up(1))
    zsend(0, other, up_all.at[other], 1)
    fwd(0, 1, y)
    load(3).wait()
    for i in range(stack):
        load(10 + i).wait()
    sent(esend, ssend.at[2])
    recv(inc.at[1 - y], ssend.at[2], srecv.at[1])

    ph = mine // 2
    fr = min(128, ph)

    def finish(base):

        def part(t, carry):
            at = pl.ds(pl.multiple_of(base + t * fr, fr), fr)
            for h in range(heads):
                qd = q_v[at, h * DK : (h + 1) * DK]
                r = ret[at, h * DV : (h + 1) * DV] + jnp.concatenate([dot(qd, inc[0, h]), dot(qd, inc[1, h])], axis=1)
                normed = r * lax.rsqrt(jnp.mean(r * r, axis=1, keepdims=True) + EPS)
                g = g_v[at, h * DV : (h + 1) * DV].astype(F32)
                g_v[at, h * DV : (h + 1) * DV] = (g / (1.0 + jnp.exp(-g)) * normed).astype(BF16)
            return carry

        lax.fori_loop(0, ph // fr, part, 0)

    pt = min(512, wc)

    def project(base, put):
        rows_at = pl.ds(pl.multiple_of(base, ph), ph)
        for i in range(stack):
            def part(t, carry, i=i):
                at = pl.ds(pl.multiple_of(t * pt, pt), pt)
                to = pl.ds(pl.multiple_of(i * wc + t * pt, pt), pt)
                put(to, dot(g_v[rows_at, :], wide[i * hv : (i + 1) * hv, at]))
                return carry

            lax.fori_loop(0, wc // pt, part, 0)

    def for_sibling(j, p):
        base = (xat(j) * 2 + (1 - c)) * mine + p * ph
        finish(base)
        mid = pl.ds(p * ph, ph)

        def put(at, val):
            pp[j, mid, at] = val.astype(BF16)

        project(base, put)
        send(pp.at[j, mid], pr.at[j, mid], psend.at[j], precv.at[j, p], to_c, track=False)

    def for_mine(j, p):
        base = (xat(j) * 2 + c) * mine + p * ph
        finish(base)
        mid = pl.ds(p * ph, ph)

        def put(at, val):
            acc[mid, at] = val.astype(BF16).astype(F32)

        project(base, put)
        recv(pr.at[j, mid], psend.at[j], precv.at[j, p])
        if j:
            for r in range(p * ROWS // 2, (p + 1) * ROWS // 2):
                at = pl.ds(r * rc, rc)
                psum[j - 1, at, :] = (acc[at, :] + pr[j, at, :].astype(F32)).astype(BF16)
                send(psum.at[j - 1, at], xr.at[j - 1, at], xsend.at[j - 1], xrecv.at[j - 1, r], to_x(j), track=False)

    for j in range(1, X):
        for p in range(2):
            for_sibling(j, p)
            for_mine(j, p)
    fwd(0, 1, 1 - y)
    for p in range(2):
        for_sibling(0, p)
        for_mine(0, p)
    recv_y(1)
    for way in range(2):
        zsend(1, other, dn_all.at[other], way)
    fwd(0, 2, y)

    for j in range(X):
        sent(pp.at[j], psend.at[j])
        if j:
            sent(psum.at[j - 1], xsend.at[j - 1])

    load(4).wait()
    for r in range(ROWS):
        at = pl.ds(r * rc, rc)
        s = acc[at, :] + pr[0, at, :].astype(F32)
        for j in range(1, X):
            recv(xr.at[j - 1, at], xsend.at[j - 1], xrecv.at[j - 1, r])
            s = s + xr[j - 1, at, :].astype(F32)
        u = (res_v[at, :].astype(F32) + s).astype(BF16)
        upd[at, :] = u
        u = u.astype(F32)
        u = u * lax.rsqrt(jnp.mean(u * u, axis=1, keepdims=True) + EPS)
        x_all[c, y, x, at, :] = (u * gain[...].astype(F32).reshape(1, d)).astype(BF16)
        own = x_all.at[c, y, x, at]
        send(own, own, asend.at[0, 0], ary.at[0, r], to_y, track=False)
        for j in range(1, X):
            send(own, own, asend.at[1, j], arx.at[j, r], to_x(j), track=False)
        send(own, own, asend.at[2, 0], ard.at[0, 0], to_c, track=False)

    load(5).wait()
    for k in range(1, Z - 1):
        if k == 1:
            continue
        fwd(0, k, 1 - y)
        if k > 2:
            fwd(0, k, y)

    ht = min(512, half)

    def hid_rows(yy, xx):
        return pl.ds(pl.multiple_of((yy * X + xx) * mine, mine), mine)

    def hid_of(cc):
        return pl.ds(pl.multiple_of(cc * half, half), half)

    def hidden(yy, xx):
        def part(t, carry):
            at = pl.ds(pl.multiple_of(t * ht, ht), ht)
            w = up_all[:, :, at].reshape(d, ht)
            for cc in range(2):
                pre = jnp.maximum(dot(x_all[cc, yy, xx], w), 0.0)
                col = pl.ds(pl.multiple_of(cc * half + t * ht, ht), ht)
                wide[hid_rows(yy, xx), col] = (pre * pre).astype(BF16)
            return carry

        lax.fori_loop(0, half // ht, part, 0)

    for i in range(X):
        for kind, yy in ((0, y), (2, y), (3, 1 - y)):
            sent(x_all.at[c, yy, xat(-i)], asend.at[kind, i])
        if i:
            sent(x_all.at[c, y, x], asend.at[1, i])

    def from_sibling(yrel, i):
        recv(x_all.at[1 - c, (1 - y) if yrel else y, xat(-i)], asend.at[2, 0], ard.at[yrel, i])

    def pass_on(yrel, i, r):
        at = pl.ds(r * rc, rc)
        ref = x_all.at[c, (1 - y) if yrel else y, xat(-i), at]
        if yrel:
            recv(ref, asend.at[0, 0], ary.at[i, r])
        else:
            recv(ref, asend.at[1, i], arx.at[i, r])
            send(ref, ref, asend.at[0, i], ary.at[i, r], to_y, track=False)
        send(ref, ref, asend.at[2 + yrel, i], ard.at[yrel, i], to_c, track=False)

    for r in range(ROWS):
        pass_on(1, 0, r)
    for r in range(ROWS):
        for j in range(1, X):
            pass_on(0, j, r)
        if r == 1:
            fwd(1, 1, 0)
    fwd(1, 1, 1)
    for k in range(n_sp):
        settle(0, k)
    from_sibling(0, 0)
    hidden(y, x)
    from_sibling(1, 0)
    hidden(1 - y, x)
    for j in range(1, X):
        for r in range(ROWS):
            pass_on(1, j, r)
        from_sibling(0, j)
        hidden(y, xat(-j))
    for j in range(1, X):
        from_sibling(1, j)
        hidden(1 - y, xat(-j))

    load(6).wait()
    m = jnp.minimum(z, Z - 1 - z)
    hm = mine // 2

    def block_of(s):
        i = s // 2
        near = jnp.where(i % 2 == 1, z - (i + 1) // 2, z + i // 2)
        far = jnp.where(z <= Z - 1 - z, i, Z - 1 - i)
        return jnp.where(i <= 2 * m, near, far) * 2 + s % 2

    units = n_sp - 1 if halves else n_sp
    total = units + 2 if halves else units
    na, nb = 3 * X - 2, X

    class Unit:
        def __init__(self, t, part=None):
            self.t, self.u, self.part = t, (t if part is None else n_sp - 1), part
            self.w = cols if part is None else cw
            self.c0 = 0 if part is None else part * cw
            self.block = block_of(self.u)

        def trim(self, ref, start):
            return ref if self.w == cols else ref.at[..., pl.ds(start, self.w)]

        def bulk(self, n, ss, rs):
            ref = wide.at[pl.ds(0, n * hm), pl.ds(0, self.w)]
            return rcopy(ref, ref, ss, rs, to_c)

        def to_sib(self):
            t = self.t
            return rcopy(self.trim(pd.at[t % 2], 0), self.trim(r1.at[self.u], self.c0), dsem.at[t % 2], drecv.at[t], to_c)

        def copies(self, stage):
            q, t, u = qs.at[self.t % SLOTS], self.t, self.u
            if stage == 0:
                pairs = [(q.at[1 - y, :, 0], r2y.at[u], to_y)]
                pairs += [(q.at[:, xat(j), 1], r2x.at[u, j - 1], to_x(j)) for j in range(1, X)]
            else:
                pairs = [(q.at[1 - y, x, 1], r3y.at[u], to_y)]
                pairs += [(q.at[y, xat(j), 0], r3x.at[u, j - 1], to_x(j)) for j in range(1, X)]
            if self.part is not None:
                to = [(1, 0, to_y)] + [(0, j, to_x(j)) for j in range(1, X)] + [(1, j, to_diag(j)) for j in range(1, X)]
                pairs = [(q.at[(1 - y) if f else y, xat(j)], rd.at[self.part, f * X + j], dev) for f, j, dev in to]
            for src, dst, dev in pairs:
                dst = dst if self.part is not None else self.trim(dst, self.c0)
                rcopy(self.trim(src, 0), dst, qsem.at[stage, t % SLOTS], qrecv.at[stage, t], dev).start()

        def wait_sib(self):
            ref = self.trim(pd.at[self.t % 2], 0)
            rcopy(ref, ref, dsem.at[self.t % 2], drecv.at[self.t], to_c).wait_send()

        def arrive(self, i):
            r0, nr, c0 = pieces[i]

            @pl.when(jnp.logical_not(has_up & has_dn))
            def _():
                ref = dn_all.at[self.block, pl.ds(r0, nr), pl.ds(c0, cw)]
                recv(ref, wsend.at[1, 0], wlast.at[i])

        def product(self, cls, r0, nr):
            w = dn_all[self.block, r0 : r0 + nr, self.c0 : self.c0 + self.w]
            return dot(wide[:, pl.ds(pl.multiple_of(cls * half + r0, 128), nr)], w)

        def compute(self, before):
            if self.part is None:
                settle(1, self.block)
            else:
                self.arrive(0)
            before()
            self.offer(self.product(1 - c, 0, half))
            ret[: 2 * X * mine, : self.w] = self.product(c, 0, half)

        def offer(self, value):
            pd[self.t % 2, :, :, :, :, : self.w] = value.astype(BF16).reshape(2, X, 2, hm, self.w)
            self.to_sib().start()

        def early(self):
            self.arrive(1)
            ret[: 2 * X * mine, cw : 2 * cw] = self.product(1 - c, 0, ka)
            ret[: 2 * X * mine, 2 * cw : 3 * cw] = self.product(c, 0, ka)

        def late(self, before):
            self.arrive(2)
            before()
            self.offer(ret[: 2 * X * mine, cw : 2 * cw] + self.product(1 - c, ka, half - ka))
            ret[: 2 * X * mine, :cw] = ret[: 2 * X * mine, 2 * cw : 3 * cw] + self.product(c, ka, half - ka)

        def first(self):
            k, at = self.t % SLOTS, slice(self.c0, self.c0 + self.w)
            self.to_sib().wait_recv()
            own = ret[: 2 * X * mine, : self.w].reshape(2, X, 2, hm, self.w)
            qs[k, :, :, :, :, : self.w] = (own.astype(BF16).astype(F32) + r1[self.u, :, :, :, :, at].astype(F32)).astype(BF16)
            self.copies(0)

        def second(self):
            k, at, w = self.t % SLOTS, slice(self.c0, self.c0 + self.w), self.w
            self.bulk(na, qsem.at[0, 0], qrecv.at[0, self.t]).wait_recv()
            qs[k, y, :, 0, :, :w] = (qs[k, y, :, 0, :, :w].astype(F32) + r2y[self.u, :, :, at].astype(F32)).astype(BF16)
            s = qs[k, :, x, 1, :, :w].astype(F32)
            for j in range(1, X):
                s = s + r2x[self.u, j - 1, :, :, at].astype(F32)
            qs[k, :, x, 1, :, :w] = s.astype(BF16)
            self.copies(1)

        def put(self):
            at = pl.ds(pl.multiple_of(self.block * cols + self.c0, 128), self.w)
            return pltpu.make_async_copy(self.trim(out.at[self.t % 4], 0), out_h.at[:, at], osem.at[self.t % 4])

        def final(self):
            k, at, w = self.t % SLOTS, slice(self.c0, self.c0 + self.w), self.w
            o = self.t % 4
            col = pl.ds(pl.multiple_of(self.block * cols + self.c0, 128), w)
            if self.part is not None:
                every = (2 * X - 1) * 2
                self.bulk(every, qsem.at[0, 0], qrecv.at[0, self.t]).wait_recv()
                s = qs[k, y, x, :, :, :w].astype(F32)
                for i in range(1, 2 * X):
                    s = s + rd[self.part, i].astype(F32)
                out[o, :, :w] = (upd[:, col].astype(F32) + s.reshape(mine, w)).astype(BF16)
                self.put().start()
                self.bulk(every, qsem.at[0, k], qrecv.at[0, 0]).wait_send()
                return
            self.bulk(nb, qsem.at[1, 0], qrecv.at[1, self.t]).wait_recv()
            s = upd[:hm, col].astype(F32) + qs[k, y, x, 0, :, :w].astype(F32)
            for j in range(1, X):
                s = s + r3x[self.u, j - 1, :, at].astype(F32)
            out[o, :hm, :w] = s.astype(BF16)
            s = upd[hm:, col].astype(F32) + qs[k, y, x, 1, :, :w].astype(F32) + r3y[self.u, :, at].astype(F32)
            out[o, hm:, :w] = s.astype(BF16)
            self.put().start()
            self.bulk(na, qsem.at[0, k], qrecv.at[0, 0]).wait_send()
            self.bulk(nb, qsem.at[1, k], qrecv.at[1, 0]).wait_send()

    last = [(2 * (k - 2 + yy), relays(1, k, yy)) for k in range(2, Z - 1) for yy in range(2)]

    def step(s, carry):
        for at, parts in last:
            for cond, go in parts:
                pl.when(cond & (s == at))(go)
        Unit(s).compute(lambda: pl.when(s >= 2)(lambda: Unit(s - 2).wait_sib()))

        @pl.when(s >= 2)
        def _():
            Unit(s - 2).second()

        Unit(s).first()

        @pl.when(s >= 4)
        def _():
            pl.when(s >= 8)(lambda: Unit(s - 8).put().wait())
            Unit(s - 4).final()

        return carry

    lax.fori_loop(0, units, step, 0)
    tail = [Unit(t) for t in range(units)]

    def finish_unit(t):
        if t >= 4:
            tail[t - 4].put().wait()
        tail[t].final()

    if halves:
        tail += [Unit(units + p, p) for p in range(2)]
        one, two = tail[units], tail[units + 1]
        one.compute(tail[units - 2].wait_sib)
        tail[units - 2].second()
        two.early()
        one.first()
        finish_unit(units - 4)
        two.late(tail[units - 1].wait_sib)
        tail[units - 1].second()
        two.first()
        finish_unit(units - 3)
    else:
        tail[units - 2].second()
        tail[units - 1].second()
    for t in range(total - 4, total):
        finish_unit(t)
    for t in range(total - 4, total):
        tail[t].put().wait()
    for t in range(total - 2, total):
        tail[t].wait_sib()
    for cond, end in pending:
        if cond is None:
            end()
        else:
            pl.when(cond)(end)


def body(n_sp, n_tp, resid, queries, keys, values, gates, log_decay, w_out, gain, up, down):
    X, Z = n_tp // 2, n_sp // 2
    rows, heads = queries.shape[0], log_decay.shape[0]
    mine, d = resid.shape
    half, cols, part = up.shape[1] // 2, down.shape[1], up.shape[0]
    freq = 10000.0 ** (-np.arange(0, DK, 2, dtype=np.float64) / DK)
    near = np.arange(BLOCK)[:, None] * freq[None, :]
    far = (BLOCK * np.arange(rows * n_sp // BLOCK))[:, None] * freq[None, :]
    tables = [jnp.asarray(np.stack([np.cos(a), np.sin(a)]), F32) for a in (near, far)]
    vm, anym = pl.BlockSpec(memory_space=pltpu.VMEM), pl.BlockSpec(memory_space=pl.ANY)
    dma = pltpu.SemaphoreType.DMA
    V = pltpu.VMEM
    hd, hv = heads * DK, heads * DV
    sq = (DK, DV // 2)
    scratch = [
        V((heads, rows), F32), *[V(t.shape, F32) for t in tables], V((4, mine, cols), BF16),
        V((rows, hd), BF16), V((rows, hd), BF16), V((rows, hv), BF16), V((rows, hv), BF16),
        V((2 * X * mine, 2 * half), BF16), V((mine, d), BF16),
        V((heads, rows, DK), BF16), V((rows, DK), BF16),
        V((2, heads, *sq), F32), V((2, heads, *sq), BF16), V((DK, DV), F32),
        V((heads, *sq), BF16), V((8, DV // 2), F32), V((8, DV // 2), F32),
        V((heads, *sq), BF16), V((heads, *sq), BF16), V((heads, *sq), BF16), V((2, heads, *sq), BF16),
        V((rows, hv), F32),
        V((X, mine, d), BF16), V((X, mine, d), BF16), V((X - 1, mine, d), BF16), V((X - 1, mine, d), BF16),
        V((mine, d), F32), V((mine, d), BF16),
        V((2, 2, X, mine, d), BF16), V((n_sp, part, half), BF16), V((n_sp, half, cols), BF16),
        V((2, 2, X, 2, mine // 2, cols), BF16),
        V((SLOTS, 2, X, 2, mine // 2, cols), BF16), V((n_sp, 2, X, 2, mine // 2, cols), BF16),
        V((n_sp, X, mine // 2, cols), BF16), V((n_sp, X - 1, 2, mine // 2, cols), BF16),
        V((n_sp, mine // 2, cols), BF16), V((n_sp, X - 1, mine // 2, cols), BF16),
        V((2, 2 * X, 2, mine // 2, cols // 2), BF16),
        dma((10 + 2 * X * mine // hv,)), dma((2, n_sp + 2)), dma((2, n_sp)), dma((3,)), dma((2,)), dma((2,)),
        dma((4,)), dma((3 + heads,)), dma((X,)), dma((X, 2)), dma((X - 1,)), dma((X - 1, ROWS)),
        dma((4, X)), dma((X, ROWS)), dma((X, ROWS)), dma((2, X)),
        dma((2,)), dma((n_sp + 1,)), dma((2, SLOTS)), dma((2, n_sp + 1)), dma((4,)),
    ]
    return pl.pallas_call(
        functools.partial(kernel, n_sp, n_tp),
        in_specs=[anym] * 7 + [vm] + [anym] * 4,
        out_specs=anym,
        out_shape=jax.ShapeDtypeStruct((mine, d), BF16),
        scratch_shapes=scratch,
        compiler_params=pltpu.CompilerParams(
            collective_id=0, has_side_effects=True, vmem_limit_bytes=67043328
        ),
        name="layer",
    )(resid, queries, keys, values, gates, log_decay, w_out, gain, up, down, *tables)


def solution(mesh):
    placed = (
        P(("sp", "tp"), None),
        P("sp", "tp"),
        P("sp", "tp"),
        P("sp", "tp"),
        P("sp", "tp"),
        P("tp", "sp"),
        P("tp", None),
        P(),
        P("sp", "tp"),
        P("tp", "sp"),
    )
    return jax.shard_map(
        functools.partial(body, mesh.shape["sp"], mesh.shape["tp"]),
        mesh=mesh,
        in_specs=placed,
        out_specs=P(("sp", "tp"), None),
        check_vma=False,
    )
```

```python
import functools

import jax
import jax.numpy as jnp
import numpy as np
from jax import lax
from jax.experimental import pallas as pl
from jax.experimental.pallas import tpu as pltpu
from jax.sharding import PartitionSpec as P

DK = 256
DV = 512
BLOCK = 128
SPAN = 256
ROWS = 4
SLOTS = 5
EPS = 1e-06
F32 = jnp.float32
BF16 = jnp.bfloat16
MESH = pl.DeviceIdType.MESH


def dot(a, b):
    return jnp.dot(a, b, preferred_element_type=F32)


def cumulative(row):
    n = row.shape[1]
    i = lax.broadcasted_iota(jnp.int32, (n, n), 0)
    j = lax.broadcasted_iota(jnp.int32, (n, n), 1)
    col = jnp.sum(jnp.where(i == j, row, 0.0), axis=1, keepdims=True)
    cum_col = jnp.sum(jnp.where(j <= i, row, 0.0), axis=1, keepdims=True)
    cum_row = jnp.sum(jnp.where(i <= j, col, 0.0), axis=0, keepdims=True)
    total = jnp.sum(row, axis=1, keepdims=True)
    return i, j, cum_col, cum_row, total


def kernel(
    n_sp, n_tp,
    resid_h, q_h, k_h, v_h, g_h, ld_h, wo_h, gain, up_h, dn_h, low_h, high_h,
    out,
    ld, low, high, q_v, k_v, v_v, g_v, wide, res_v, kr, kd, stf, sth, strun, yst, tot, ytot, crecv, csend, esend, inc, ret,
    pp, pr, psum, xr, acc, upd, x_all, up_all, dn_all, pd, qs, r1, r2y, r2x, r3y, r3x, rd,
    lsem, wsend, wrecv, wlast, wysend, wyrecv, ssend, srecv, psend, precv, xsend, xrecv,
    asend, arx, ary, ard, dsem, drecv, qsem, qrecv,
):
    Z, X = n_sp // 2, n_tp // 2
    sp, tp = lax.axis_index("sp"), lax.axis_index("tp")
    z, y = sp // 2, sp % 2
    x, c = tp // 2, tp % 2
    rows = k_v.shape[0]
    heads = kr.shape[0]
    mine = res_v.shape[0]
    d = res_v.shape[1]
    half = up_all.shape[2]
    cols = dn_all.shape[2]
    nblk, nspan = rows // BLOCK, rows // SPAN
    rc = mine // ROWS
    has_up, has_dn = z < Z - 1, z > 0
    halves = cols % 256 == 0 and Z > 2
    cw, ka = cols // 2, half - min(256, half // 2)
    pieces = ((0, half, 0), (0, ka, cw), (ka, half - ka, cw))

    def rcopy(src, dst, ss, rs, dev):
        return pltpu.make_async_remote_copy(src, dst, ss, rs, device_id=dev, device_id_type=MESH)

    to_zp, to_zm = {"sp": sp + 2}, {"sp": sp - 2}
    to_y = {"sp": z * 2 + (1 - y)}
    to_c = {"tp": x * 2 + (1 - c)}

    def xat(j):
        return lax.rem(x + j + X, X)

    def to_x(j):
        return {"tp": xat(j) * 2 + c}

    def to_diag(j):
        return {"sp": z * 2 + (1 - y), "tp": xat(j) * 2 + c}

    pending = []

    def send(src, dst, ss, rs, dev, cond=None, track=True):
        def go():
            rcopy(src, dst, ss, rs, dev).start()

        if cond is None:
            go()
        else:
            pl.when(cond)(go)
        if track:
            sent(src, ss, cond)

    def sent(ref, ss, cond=None):
        pending.append((cond, lambda: rcopy(ref, ref, ss, ss, to_c).wait_send()))

    def recv(dst, ss, rs):
        rcopy(dst, dst, ss, rs, to_c).wait_recv()

    loads = [
        (k_h, k_v), (v_h, v_v), (q_h, q_v), (g_h, g_v), (resid_h, res_v),
        (up_h.at[:, pl.ds(pl.multiple_of(y * half, half), half)], up_all.at[sp]),
        (dn_h.at[pl.ds(pl.multiple_of(y * half, half), half), :], dn_all.at[sp]),
    ]
    hv = v_v.shape[1]
    stack = wide.shape[0] // hv
    wc = d // stack
    loads += [(ld_h, ld), (low_h, low), (high_h, high)]
    loads += [(wo_h.at[:, pl.ds(i * wc, wc)], wide.at[pl.ds(i * hv, hv)]) for i in range(stack)]

    def load(i):
        return pltpu.make_async_copy(loads[i][0], loads[i][1], lsem.at[i])

    for i in (7, 8, 9, 0, 1):
        load(i).start()

    barrier = pltpu.get_barrier_semaphore()
    greet = [(to_y, None), (to_c, None)] + [(to_x(j), None) for j in range(1, X)]
    if halves:
        greet += [(to_diag(j), None) for j in range(1, X)]
    greet += [(to_zp, has_up), (to_zm, has_dn)]
    for dev, cond in greet:
        def hello(dev=dev):
            pl.semaphore_signal(barrier, 1, device_id=dev, device_id_type=MESH)
        if cond is None:
            hello()
        else:
            pl.when(cond)(hello)
    pl.semaphore_wait(barrier, X + 1 + halves * (X - 1) + jnp.where(has_up, 1, 0) + jnp.where(has_dn, 1, 0))

    h_up = up_h.at[:, pl.ds(pl.multiple_of(y * half, half), half)]
    h_dn = dn_h.at[pl.ds(pl.multiple_of(y * half, half), half), :]
    o_up = up_h.at[:, pl.ds(pl.multiple_of((1 - y) * half, half), half)]
    o_dn = dn_h.at[pl.ds(pl.multiple_of((1 - y) * half, half), half), :]
    alls = (up_all, dn_all)

    def zsend(w, piece, src, way):
        dev, cond = ((to_zp, has_up), (to_zm, has_dn))[way]
        send(src, alls[w].at[piece], wsend.at[way, 0], wrecv.at[w, piece], dev, cond, track=False)

    late = z >= 2
    early = jnp.logical_not(late)
    for way in range(2):
        zsend(0, sp, h_up, way)
    zsend(1, sp, h_dn, 1)

    def own_dn():
        return rcopy(h_dn, dn_all.at[sp], wsend.at[0, 0], wrecv.at[1, sp], to_zp)

    @pl.when(late & has_up)
    def _():
        own_dn().start()

    for way, cond in enumerate((has_up, has_dn)):
        sent(up_all.at[pl.ds(0, 4)], wsend.at[way, 0], cond)
    hr = up_h.shape[0] // 2
    other = z * 2 + (1 - y)

    def ysend(w, src):
        send(src, alls[w].at[sp], wysend.at[w], wyrecv.at[w], to_y)

    def recv_y(w):
        recv(alls[w].at[other], wysend.at[w], wyrecv.at[w])

    def relays(w, k, yy):
        parts = []
        low, high = (z - k) * 2 + yy, (z + k) * 2 + yy
        for piece, way, cond in ((low, 0, (z >= k) & has_up), (high, 1, (z + k < Z) & has_dn)):
            ref, sem, dev = alls[w].at[piece], wsend.at[way, k], (to_zp, to_zm)[way]

            def go(ref=ref, sem=sem, dev=dev, piece=piece):
                recv(ref, sem, wrecv.at[w, piece])
                if halves and (w, k, yy) == (1, Z - 2, 1):
                    for h, (r0, nr, c0) in enumerate(pieces):
                        part = ref.at[pl.ds(r0, nr), pl.ds(c0, cw)]
                        rcopy(part, part, sem, wlast.at[h], dev).start()
                else:
                    rcopy(ref, ref, sem, wrecv.at[w, piece], dev).start()

            if (w, yy) == (1, 1):
                sent(up_all.at[pl.ds(0, 4)], sem, cond)
            parts.append((cond, go))
        return parts

    def fwd(w, k, yy):
        if k <= Z - 2:
            for cond, go in relays(w, k, yy):
                pl.when(cond)(go)

    def settle(w, piece):
        plane = piece // 2
        cond = ((plane < z) & jnp.logical_not(has_up)) | ((plane > z) & jnp.logical_not(has_dn))

        @pl.when(cond)
        def _():
            recv(alls[w].at[piece], wsend.at[0, 0], wrecv.at[w, piece])

    def angles(b):
        at = sp * nblk + b
        hc, hs = high[0, pl.ds(at, 1), :], high[1, pl.ds(at, 1), :]
        lc, ls = low[0], low[1]
        return hc * lc - hs * ls, hs * lc + hc * ls

    def rotated(blk, co, si):
        a, b = blk[:, : DK // 2].astype(F32), blk[:, DK // 2 :].astype(F32)
        return jnp.concatenate([a * co - b * si, a * si + b * co], axis=1)

    tot[...] = jnp.zeros_like(tot)
    for i in (2, 3, *range(10, len(loads)), 4, 5, 6):
        load(i).start()
    for i in (7, 8, 9, 0):
        load(i).wait()
    for h in range(heads):
        def state_block(t, after, h=h):
            b = nblk - 1 - t
            at = pl.ds(pl.multiple_of(b * BLOCK, BLOCK), BLOCK)
            row = ld[h : h + 1, pl.ds(pl.multiple_of(b * BLOCK, BLOCK), BLOCK)]
            i, j, cum_col, _, total = cumulative(row)
            co, si = angles(b)
            key = (rotated(k_v[at, h * DK : (h + 1) * DK], co, si) * DK ** (-0.5)).astype(BF16)
            kr[h, at, :] = key
            kd[at, :] = (key.astype(F32) * jnp.exp(total - cum_col + after)).astype(BF16)
            return after + total

        whole = lax.fori_loop(0, nblk, state_block, jnp.zeros((1, 1), F32))
        tot[h : h + 1, :] = jnp.broadcast_to(jnp.exp(whole), (1, tot.shape[1]))
        if h == 0:
            load(1).wait()
        s = lax.dot_general(kd[...], v_v[:, h * DV : (h + 1) * DV], (((0,), (0,)), ((), ())), preferred_element_type=F32)
        for p in range(2):
            part = s[:, p * DV // 2 : (p + 1) * DV // 2]
            stf[p, h] = part
            sth[p, h] = part.astype(BF16)
        send(sth.at[1 - y, h], yst.at[h], ssend.at[0], srecv.at[0], to_y, track=False)
    sent(sth.at[1 - y], ssend.at[0])
    send(tot, ytot, ssend.at[3], srecv.at[2], to_y)
    ysend(0, o_up)
    ysend(1, o_dn)

    load(2).wait()

    def local(h):
        strun[...] = jnp.zeros_like(strun)

        def span(t, before):
            at = pl.ds(pl.multiple_of(t * SPAN, SPAN), SPAN)
            row = ld[h : h + 1, pl.ds(pl.multiple_of(t * SPAN, SPAN), SPAN)]
            i, j, cum_col, cum_row, total = cumulative(row)
            parts = []
            for u in range(SPAN // BLOCK):
                co, si = angles(t * (SPAN // BLOCK) + u)
                qat = pl.ds(pl.multiple_of(t * SPAN + u * BLOCK, BLOCK), BLOCK)
                parts.append(rotated(q_v[qat, h * DK : (h + 1) * DK], co, si))
            query = jnp.concatenate(parts, axis=0).astype(BF16)
            key = kr[h, at, :]
            factor = jnp.where(i >= j, jnp.exp(jnp.minimum(cum_col - cum_row, 0.0)), 0.0)
            scores = lax.dot_general(query, key, (((1,), (1,)), ((), ())), preferred_element_type=F32)
            weights = (scores * factor).astype(BF16)
            q32 = query.astype(F32)
            val = v_v[at, h * DV : (h + 1) * DV]
            ret[at, h * DV : (h + 1) * DV] = dot(weights, val) + dot((q32 * jnp.exp(cum_col)).astype(BF16), strun[...].astype(BF16))
            q_v[at, h * DK : (h + 1) * DK] = (q32 * jnp.exp(cum_col + before)).astype(BF16)
            kdec = (key.astype(F32) * jnp.exp(total - cum_col)).astype(BF16)
            strun[...] = jnp.exp(total) * strun[...] + lax.dot_general(
                kdec, val, (((0,), (0,)), ((), ())), preferred_element_type=F32
            )
            return before + total

        lax.fori_loop(0, nspan, span, jnp.zeros((1, 1), F32))

    local(0)

    first = y == 0
    recv(ytot, ssend.at[3], srecv.at[2])
    recv(yst, ssend.at[0], srecv.at[0])

    def decays(h):
        own, oth = tot[h : h + 1, : DV // 2], ytot[h : h + 1, : DV // 2]
        return jnp.where(first, own, oth), jnp.where(first, oth, own)

    @pl.when(jnp.logical_not(has_dn))
    def _():
        crecv[...] = jnp.zeros_like(crecv)

    def s_pair(h):
        own, oth = stf[y, h], yst[h].astype(F32)
        return jnp.where(first, own, oth), jnp.where(first, oth, own)

    def chain(h):
        d0, d1 = decays(h)
        s0, s1 = s_pair(h)
        csend[h] = (d0 * d1 * crecv[h].astype(F32) + (d1 * s0 + s1)).astype(BF16)

    def chain_send(h):
        rcopy(csend.at[h], crecv.at[h], ssend.at[1], srecv.at[3 + h], to_zp).start()

    @pl.when(jnp.logical_not(has_dn))
    def _():
        for h in range(heads):
            chain(h)
            chain_send(h)
        own_dn().start()

    for h in range(1, heads):
        local(h)

    def part_up(part):
        ref = up_all.at[other, pl.ds(part * hr, hr)]
        rcopy(ref, ref, wsend.at[0, 0], wrecv.at[0, other], to_zp).start()

    @pl.when(late)
    def _():
        recv_y(0)
        pl.when(has_up)(lambda: part_up(0))

    @pl.when(has_dn)
    def _():
        for h in range(heads):
            recv(crecv.at[h], ssend.at[1], srecv.at[3 + h])

            @pl.when(has_up)
            def _():
                chain(h)
                chain_send(h)

        @pl.when(early & has_up)
        def _():
            own_dn().start()

    def chain_end():
        rcopy(csend, crecv, ssend.at[1], srecv.at[0], to_zp).wait_send()

    pending.append((has_up, chain_end))
    for h in range(heads):
        d0, _ = decays(h)
        s0, _ = s_pair(h)
        got = crecv[h].astype(F32)
        later = (d0 * got + s0).astype(BF16)
        inc[y, h] = jnp.where(first, crecv[h], later)
        esend[h] = jnp.where(first, later, crecv[h])
        send(esend.at[h], inc.at[y, h], ssend.at[2], srecv.at[1], to_y, track=False)
    @pl.when(early)
    def _():
        recv_y(0)
        pl.when(has_up)(lambda: part_up(0))

    pl.when(has_up)(lambda: part_up(1))
    zsend(0, other, up_all.at[other], 1)
    fwd(0, 1, y)
    load(3).wait()
    for i in range(stack):
        load(10 + i).wait()
    sent(esend, ssend.at[2])
    recv(inc.at[1 - y], ssend.at[2], srecv.at[1])

    ph = mine // 2
    fr = min(128, ph)

    def finish(base):

        def part(t, carry):
            at = pl.ds(pl.multiple_of(base + t * fr, fr), fr)
            for h in range(heads):
                qd = q_v[at, h * DK : (h + 1) * DK]
                r = ret[at, h * DV : (h + 1) * DV] + jnp.concatenate([dot(qd, inc[0, h]), dot(qd, inc[1, h])], axis=1)
                normed = r * lax.rsqrt(jnp.mean(r * r, axis=1, keepdims=True) + EPS)
                g = g_v[at, h * DV : (h + 1) * DV].astype(F32)
                g_v[at, h * DV : (h + 1) * DV] = (g / (1.0 + jnp.exp(-g)) * normed).astype(BF16)
            return carry

        lax.fori_loop(0, ph // fr, part, 0)

    pt = min(512, wc)

    def project(base, put):
        rows_at = pl.ds(pl.multiple_of(base, ph), ph)
        for i in range(stack):
            def part(t, carry, i=i):
                at = pl.ds(pl.multiple_of(t * pt, pt), pt)
                to = pl.ds(pl.multiple_of(i * wc + t * pt, pt), pt)
                put(to, dot(g_v[rows_at, :], wide[i * hv : (i + 1) * hv, at]))
                return carry

            lax.fori_loop(0, wc // pt, part, 0)

    def for_sibling(j, p):
        base = (xat(j) * 2 + (1 - c)) * mine + p * ph
        finish(base)
        mid = pl.ds(p * ph, ph)

        def put(at, val):
            pp[j, mid, at] = val.astype(BF16)

        project(base, put)
        send(pp.at[j, mid], pr.at[j, mid], psend.at[j], precv.at[j, p], to_c, track=False)

    def for_mine(j, p):
        base = (xat(j) * 2 + c) * mine + p * ph
        finish(base)
        mid = pl.ds(p * ph, ph)

        def put(at, val):
            acc[mid, at] = val.astype(BF16).astype(F32)

        project(base, put)
        recv(pr.at[j, mid], psend.at[j], precv.at[j, p])
        if j:
            for r in range(p * ROWS // 2, (p + 1) * ROWS // 2):
                at = pl.ds(r * rc, rc)
                psum[j - 1, at, :] = (acc[at, :] + pr[j, at, :].astype(F32)).astype(BF16)
                send(psum.at[j - 1, at], xr.at[j - 1, at], xsend.at[j - 1], xrecv.at[j - 1, r], to_x(j), track=False)

    for j in range(1, X):
        for p in range(2):
            for_sibling(j, p)
            for_mine(j, p)
    fwd(0, 1, 1 - y)
    for p in range(2):
        for_sibling(0, p)
        for_mine(0, p)
    recv_y(1)
    for way in range(2):
        zsend(1, other, dn_all.at[other], way)
    fwd(0, 2, y)

    for j in range(X):
        sent(pp.at[j], psend.at[j])
        if j:
            sent(psum.at[j - 1], xsend.at[j - 1])

    load(4).wait()
    for r in range(ROWS):
        at = pl.ds(r * rc, rc)
        s = acc[at, :] + pr[0, at, :].astype(F32)
        for j in range(1, X):
            recv(xr.at[j - 1, at], xsend.at[j - 1], xrecv.at[j - 1, r])
            s = s + xr[j - 1, at, :].astype(F32)
        u = (res_v[at, :].astype(F32) + s).astype(BF16)
        upd[at, :] = u
        u = u.astype(F32)
        u = u * lax.rsqrt(jnp.mean(u * u, axis=1, keepdims=True) + EPS)
        x_all[c, y, x, at, :] = (u * gain[...].astype(F32).reshape(1, d)).astype(BF16)
        own = x_all.at[c, y, x, at]
        send(own, own, asend.at[0, 0], ary.at[0, r], to_y, track=False)
        for j in range(1, X):
            send(own, own, asend.at[1, j], arx.at[j - 1, r], to_x(j), track=False)
        send(own, own, asend.at[2, 0], ard.at[0, 0], to_c, track=False)

    load(5).wait()
    for k in range(1, Z - 1):
        if k == 1:
            continue
        fwd(0, k, 1 - y)
        if k > 2:
            fwd(0, k, y)

    ht = min(512, half)

    def hid_rows(yy, xx):
        return pl.ds(pl.multiple_of((yy * X + xx) * mine, mine), mine)

    def hid_of(cc):
        return pl.ds(pl.multiple_of(cc * half, half), half)

    def hidden(yy, xx):
        def part(t, carry):
            at = pl.ds(pl.multiple_of(t * ht, ht), ht)
            w = up_all[:, :, at].reshape(d, ht)
            for cc in range(2):
                pre = jnp.maximum(dot(x_all[cc, yy, xx], w), 0.0)
                col = pl.ds(pl.multiple_of(cc * half + t * ht, ht), ht)
                wide[hid_rows(yy, xx), col] = (pre * pre).astype(BF16)
            return carry

        lax.fori_loop(0, half // ht, part, 0)

    for i in range(X):
        for kind, yy in ((0, y), (2, y), (3, 1 - y)):
            sent(x_all.at[c, yy, xat(-i)], asend.at[kind, i])
        if i:
            sent(x_all.at[c, y, x], asend.at[1, i])

    def from_sibling(yrel, i):
        recv(x_all.at[1 - c, (1 - y) if yrel else y, xat(-i)], asend.at[2, 0], ard.at[yrel, i])

    def pass_on(yrel, i, r):
        at = pl.ds(r * rc, rc)
        ref = x_all.at[c, (1 - y) if yrel else y, xat(-i), at]
        if yrel:
            recv(ref, asend.at[0, 0], ary.at[i, r])
        else:
            recv(ref, asend.at[1, i], arx.at[i - 1, r])
            send(ref, ref, asend.at[0, i], ary.at[i, r], to_y, track=False)
        send(ref, ref, asend.at[2 + yrel, i], ard.at[yrel, i], to_c, track=False)

    for r in range(ROWS):
        pass_on(1, 0, r)
    for r in range(ROWS):
        for j in range(1, X):
            pass_on(0, j, r)
        if r == 1:
            fwd(1, 1, 0)
    fwd(1, 1, 1)
    for k in range(n_sp):
        settle(0, k)
    from_sibling(0, 0)
    hidden(y, x)
    from_sibling(1, 0)
    hidden(1 - y, x)
    for j in range(1, X):
        for r in range(ROWS):
            pass_on(1, j, r)
        from_sibling(0, j)
        hidden(y, xat(-j))
    for j in range(1, X):
        from_sibling(1, j)
        hidden(1 - y, xat(-j))

    load(6).wait()
    m = jnp.minimum(z, Z - 1 - z)
    hm = mine // 2

    def block_of(s):
        i = s // 2
        near = jnp.where(i % 2 == 1, z - (i + 1) // 2, z + i // 2)
        far = jnp.where(z <= Z - 1 - z, i, Z - 1 - i)
        return jnp.where(i <= 2 * m, near, far) * 2 + s % 2

    units = n_sp - 1 if halves else n_sp
    total = units + 2 if halves else units
    na, nb = 3 * X - 2, X

    class Unit:
        def __init__(self, t, part=None):
            self.t, self.u, self.part = t, (t if part is None else n_sp - 1), part
            self.w = cols if part is None else cw
            self.c0 = 0 if part is None else part * cw
            self.block = block_of(self.u)

        def trim(self, ref, start):
            return ref if self.w == cols else ref.at[..., pl.ds(start, self.w)]

        def bulk(self, n, ss, rs):
            ref = wide.at[pl.ds(0, n * hm), pl.ds(0, self.w)]
            return rcopy(ref, ref, ss, rs, to_c)

        def to_sib(self):
            t = self.t
            return rcopy(self.trim(pd.at[t % 2], 0), self.trim(r1.at[self.u], self.c0), dsem.at[t % 2], drecv.at[t], to_c)

        def copies(self, stage):
            q, t, u = qs.at[self.t % SLOTS], self.t, self.u
            if stage == 0:
                pairs = [(q.at[1 - y, :, 0], r2y.at[u], to_y)]
                pairs += [(q.at[:, xat(j), 1], r2x.at[u, j - 1], to_x(j)) for j in range(1, X)]
            else:
                pairs = [(q.at[1 - y, x, 1], r3y.at[u], to_y)]
                pairs += [(q.at[y, xat(j), 0], r3x.at[u, j - 1], to_x(j)) for j in range(1, X)]
            if self.part is not None:
                to = [(1, 0, to_y)] + [(0, j, to_x(j)) for j in range(1, X)] + [(1, j, to_diag(j)) for j in range(1, X)]
                pairs = [(q.at[(1 - y) if f else y, xat(j)], rd.at[self.part, f * X + j], dev) for f, j, dev in to]
            for src, dst, dev in pairs:
                dst = dst if self.part is not None else self.trim(dst, self.c0)
                rcopy(self.trim(src, 0), dst, qsem.at[stage, t % SLOTS], qrecv.at[stage, t], dev).start()

        def wait_sib(self):
            ref = self.trim(pd.at[self.t % 2], 0)
            rcopy(ref, ref, dsem.at[self.t % 2], drecv.at[self.t], to_c).wait_send()

        def arrive(self, i):
            r0, nr, c0 = pieces[i]

            @pl.when(jnp.logical_not(has_up & has_dn))
            def _():
                ref = dn_all.at[self.block, pl.ds(r0, nr), pl.ds(c0, cw)]
                recv(ref, wsend.at[0, 0], wlast.at[i])

        def product(self, cls, r0, nr):
            w = dn_all[self.block, r0 : r0 + nr, self.c0 : self.c0 + self.w]
            return dot(wide[:, pl.ds(pl.multiple_of(cls * half + r0, 128), nr)], w)

        def compute(self, before):
            if self.part is None:
                settle(1, self.block)
            else:
                self.arrive(0)
            before()
            self.offer(self.product(1 - c, 0, half))
            ret[: 2 * X * mine, : self.w] = self.product(c, 0, half)

        def offer(self, value):
            pd[self.t % 2, :, :, :, :, : self.w] = value.astype(BF16).reshape(2, X, 2, hm, self.w)
            self.to_sib().start()

        def compute_late(self, before):
            self.arrive(1)
            ret[: 2 * X * mine, cw : 2 * cw] = self.product(1 - c, 0, ka)
            before()
            self.arrive(2)
            self.offer(ret[: 2 * X * mine, cw : 2 * cw] + self.product(1 - c, ka, half - ka))
            ret[: 2 * X * mine, :cw] = self.product(c, 0, half)

        def first(self):
            k, at = self.t % SLOTS, slice(self.c0, self.c0 + self.w)
            self.to_sib().wait_recv()
            own = ret[: 2 * X * mine, : self.w].reshape(2, X, 2, hm, self.w)
            qs[k, :, :, :, :, : self.w] = (own.astype(BF16).astype(F32) + r1[self.u, :, :, :, :, at].astype(F32)).astype(BF16)
            self.copies(0)

        def second(self):
            k, at, w = self.t % SLOTS, slice(self.c0, self.c0 + self.w), self.w
            self.bulk(na, qsem.at[0, 0], qrecv.at[0, self.t]).wait_recv()
            qs[k, y, :, 0, :, :w] = (qs[k, y, :, 0, :, :w].astype(F32) + r2y[self.u, :, :, at].astype(F32)).astype(BF16)
            s = qs[k, :, x, 1, :, :w].astype(F32)
            for j in range(1, X):
                s = s + r2x[self.u, j - 1, :, :, at].astype(F32)
            qs[k, :, x, 1, :, :w] = s.astype(BF16)
            self.copies(1)

        def final(self):
            k, at, w = self.t % SLOTS, slice(self.c0, self.c0 + self.w), self.w
            col = pl.ds(pl.multiple_of(self.block * cols + self.c0, 128), w)
            if self.part is not None:
                every = (2 * X - 1) * 2
                self.bulk(every, qsem.at[0, 0], qrecv.at[0, self.t]).wait_recv()
                s = qs[k, y, x, :, :, :w].astype(F32)
                for i in range(1, 2 * X):
                    s = s + rd[self.part, i].astype(F32)
                out[:, col] = (upd[:, col].astype(F32) + s.reshape(mine, w)).astype(BF16)
                self.bulk(every, qsem.at[0, k], qrecv.at[0, 0]).wait_send()
                return
            self.bulk(nb, qsem.at[1, 0], qrecv.at[1, self.t]).wait_recv()
            s = upd[:hm, col].astype(F32) + qs[k, y, x, 0, :, :w].astype(F32)
            for j in range(1, X):
                s = s + r3x[self.u, j - 1, :, at].astype(F32)
            out[:hm, col] = s.astype(BF16)
            s = upd[hm:, col].astype(F32) + qs[k, y, x, 1, :, :w].astype(F32) + r3y[self.u, :, at].astype(F32)
            out[hm:, col] = s.astype(BF16)
            self.bulk(na, qsem.at[0, k], qrecv.at[0, 0]).wait_send()
            self.bulk(nb, qsem.at[1, k], qrecv.at[1, 0]).wait_send()

    last = [(2 * (k - 2 + yy), relays(1, k, yy)) for k in range(2, Z - 1) for yy in range(2)]

    def step(s, carry):
        for at, parts in last:
            for cond, go in parts:
                pl.when(cond & (s == at))(go)
        Unit(s).compute(lambda: pl.when(s >= 2)(lambda: Unit(s - 2).wait_sib()))

        @pl.when(s >= 2)
        def _():
            Unit(s - 2).second()

        Unit(s).first()

        @pl.when(s >= 4)
        def _():
            Unit(s - 4).final()

        return carry

    lax.fori_loop(0, units, step, 0)
    tail = [Unit(t) for t in range(units)]

    def finish_unit(t):
        tail[t].final()

    if halves:
        tail += [Unit(units + p, p) for p in range(2)]
        one, two = tail[units], tail[units + 1]
        one.compute(tail[units - 2].wait_sib)
        tail[units - 2].second()
        one.first()
        finish_unit(units - 4)
        two.compute_late(tail[units - 1].wait_sib)
        tail[units - 1].second()
        two.first()
        finish_unit(units - 3)
    else:
        tail[units - 2].second()
        tail[units - 1].second()
    for t in range(total - 4, total):
        finish_unit(t)
    for t in range(total - 2, total):
        tail[t].wait_sib()
    for cond, end in pending:
        if cond is None:
            end()
        else:
            pl.when(cond)(end)


def body(n_sp, n_tp, resid, queries, keys, values, gates, log_decay, w_out, gain, up, down):
    X, Z = n_tp // 2, n_sp // 2
    rows, heads = queries.shape[0], log_decay.shape[0]
    mine, d = resid.shape
    half, cols, part = up.shape[1] // 2, down.shape[1], up.shape[0]
    freq = 10000.0 ** (-np.arange(0, DK, 2, dtype=np.float64) / DK)
    near = np.arange(BLOCK)[:, None] * freq[None, :]
    far = (BLOCK * np.arange(rows * n_sp // BLOCK))[:, None] * freq[None, :]
    tables = [jnp.asarray(np.stack([np.cos(a), np.sin(a)]), F32) for a in (near, far)]
    vm, anym = pl.BlockSpec(memory_space=pltpu.VMEM), pl.BlockSpec(memory_space=pl.ANY)
    dma = pltpu.SemaphoreType.DMA
    V = pltpu.VMEM
    hd, hv = heads * DK, heads * DV
    sq = (DK, DV // 2)
    scratch = [
        V((heads, rows), F32), *[V(t.shape, F32) for t in tables],
        V((rows, hd), BF16), V((rows, hd), BF16), V((rows, hv), BF16), V((rows, hv), BF16),
        V((2 * X * mine, 2 * half), BF16), V((mine, d), BF16),
        V((heads, rows, DK), BF16), V((rows, DK), BF16),
        V((2, heads, *sq), F32), V((2, heads, *sq), BF16), V((DK, DV), F32),
        V((heads, *sq), BF16), V((8, DV // 2), F32), V((8, DV // 2), F32),
        V((heads, *sq), BF16), V((heads, *sq), BF16), V((heads, *sq), BF16), V((2, heads, *sq), BF16),
        V((rows, hv), F32),
        V((X, mine, d), BF16), V((X, mine, d), BF16), V((X - 1, mine, d), BF16), V((X - 1, mine, d), BF16),
        V((mine, d), F32), V((mine, d), BF16),
        V((2, 2, X, mine, d), BF16), V((n_sp, part, half), BF16), V((n_sp, half, cols), BF16),
        V((2, 2, X, 2, mine // 2, cols), BF16),
        V((SLOTS, 2, X, 2, mine // 2, cols), BF16), V((n_sp, 2, X, 2, mine // 2, cols), BF16),
        V((n_sp, X, mine // 2, cols), BF16), V((n_sp, X - 1, 2, mine // 2, cols), BF16),
        V((n_sp, mine // 2, cols), BF16), V((n_sp, X - 1, mine // 2, cols), BF16),
        V((2, 2 * X, 2, mine // 2, cols // 2), BF16),
        dma((10 + 2 * X * mine // hv,)), dma((2, max(1, n_sp // 2 - 1))), dma((2, n_sp)), dma((3,)), dma((2,)), dma((2,)),
        dma((4,)), dma((3 + heads,)), dma((X,)), dma((X, 2)), dma((X - 1,)), dma((X - 1, ROWS)),
        dma((4, X)), dma((X - 1, ROWS)), dma((X, ROWS)), dma((2, X)),
        dma((2,)), dma((n_sp + 1,)), dma((2, SLOTS)), dma((2, n_sp + 1)),
    ]
    return pl.pallas_call(
        functools.partial(kernel, n_sp, n_tp),
        in_specs=[anym] * 7 + [vm] + [anym] * 4,
        out_specs=vm,
        out_shape=pltpu.VMEM((mine, d), BF16),
        scratch_shapes=scratch,
        compiler_params=pltpu.CompilerParams(
            collective_id=0, has_side_effects=True, vmem_limit_bytes=62 * 2**20
        ),
        name="layer",
    )(resid, queries, keys, values, gates, log_decay, w_out, gain, up, down, *tables)


def solution(mesh):
    placed = (
        P(("sp", "tp"), None),
        P("sp", "tp"),
        P("sp", "tp"),
        P("sp", "tp"),
        P("sp", "tp"),
        P("tp", "sp"),
        P("tp", None),
        P(),
        P("sp", "tp"),
        P("tp", "sp"),
    )
    return jax.shard_map(
        functools.partial(body, mesh.shape["sp"], mesh.shape["tp"]),
        mesh=mesh,
        in_specs=placed,
        out_specs=P(("sp", "tp"), None),
        check_vma=False,
    )
```

```python
import functools

import jax
import jax.numpy as jnp
import numpy as np
from jax import lax
from jax.experimental import pallas as pl
from jax.experimental.pallas import tpu as pltpu
from jax.sharding import PartitionSpec as P

DK = 256
DV = 512
BLOCK = 128
SPAN = 256
ROWS = 4
SLOTS = 5
EPS = 1e-06
F32 = jnp.float32
BF16 = jnp.bfloat16
MESH = pl.DeviceIdType.MESH


def dot(a, b):
    return jnp.dot(a, b, preferred_element_type=F32)


def cumulative(row):
    n = row.shape[1]
    i = lax.broadcasted_iota(jnp.int32, (n, n), 0)
    j = lax.broadcasted_iota(jnp.int32, (n, n), 1)
    col = jnp.sum(jnp.where(i == j, row, 0.0), axis=1, keepdims=True)
    cum_col = jnp.sum(jnp.where(j <= i, row, 0.0), axis=1, keepdims=True)
    cum_row = jnp.sum(jnp.where(i <= j, col, 0.0), axis=0, keepdims=True)
    total = jnp.sum(row, axis=1, keepdims=True)
    return i, j, cum_col, cum_row, total


def kernel(
    n_sp, n_tp,
    resid_h, q_h, k_h, v_h, g_h, ld_h, wo_h, gain, up_h, dn_h, low_h, high_h,
    out,
    ld, low, high, q_v, k_v, v_v, g_v, wide, res_v, kr, kd, stf, sth, strun, yst, tot, ytot, crecv, csend, esend, inc, ret,
    pp, pr, psum, xr, acc, upd, x_all, up_all, dn_all, pd, qs, r1, r2y, r2x, r3y, r3x, rd,
    lsem, wsend, wrecv, wlast, wysend, wyrecv, ssend, srecv, psend, precv, xsend, xrecv,
    asend, arx, ary, ard, dsem, drecv, qsem, qrecv,
):
    Z, X = n_sp // 2, n_tp // 2
    sp, tp = lax.axis_index("sp"), lax.axis_index("tp")
    z, y = sp // 2, sp % 2
    x, c = tp // 2, tp % 2
    rows = k_v.shape[0]
    heads = kr.shape[0]
    mine = res_v.shape[0]
    d = res_v.shape[1]
    half = up_all.shape[2]
    cols = dn_all.shape[2]
    nblk, nspan = rows // BLOCK, rows // SPAN
    rc = mine // ROWS
    has_up, has_dn = z < Z - 1, z > 0
    halves = cols % 256 == 0 and Z > 2
    cw, ka = cols // 2, half // 2
    pieces = ((0, half, 0), (0, ka, cw), (ka, half - ka, cw))

    def rcopy(src, dst, ss, rs, dev):
        return pltpu.make_async_remote_copy(src, dst, ss, rs, device_id=dev, device_id_type=MESH)

    to_zp, to_zm = {"sp": sp + 2}, {"sp": sp - 2}
    to_y = {"sp": z * 2 + (1 - y)}
    to_c = {"tp": x * 2 + (1 - c)}

    def xat(j):
        return lax.rem(x + j + X, X)

    def to_x(j):
        return {"tp": xat(j) * 2 + c}

    def to_diag(j):
        return {"sp": z * 2 + (1 - y), "tp": xat(j) * 2 + c}

    pending = []

    def send(src, dst, ss, rs, dev, cond=None, track=True):
        def go():
            rcopy(src, dst, ss, rs, dev).start()

        if cond is None:
            go()
        else:
            pl.when(cond)(go)
        if track:
            sent(src, ss, cond)

    def sent(ref, ss, cond=None):
        pending.append((cond, lambda: rcopy(ref, ref, ss, ss, to_c).wait_send()))

    def recv(dst, ss, rs):
        rcopy(dst, dst, ss, rs, to_c).wait_recv()

    loads = [
        (k_h, k_v), (v_h, v_v), (q_h, q_v), (g_h, g_v), (resid_h, res_v),
        (up_h.at[:, pl.ds(pl.multiple_of(y * half, half), half)], up_all.at[sp]),
        (dn_h.at[pl.ds(pl.multiple_of(y * half, half), half), :], dn_all.at[sp]),
    ]
    hv = v_v.shape[1]
    stack = wide.shape[0] // hv
    wc = d // stack
    loads += [(ld_h, ld), (low_h, low), (high_h, high)]
    loads += [(wo_h.at[:, pl.ds(i * wc, wc)], wide.at[pl.ds(i * hv, hv)]) for i in range(stack)]

    def load(i):
        return pltpu.make_async_copy(loads[i][0], loads[i][1], lsem.at[i])

    for i in (7, 8, 9, 0, 1):
        load(i).start()

    barrier = pltpu.get_barrier_semaphore()
    greet = [(to_y, None), (to_c, None)] + [(to_x(j), None) for j in range(1, X)]
    if halves:
        greet += [(to_diag(j), None) for j in range(1, X)]
    greet += [(to_zp, has_up), (to_zm, has_dn)]
    for dev, cond in greet:
        def hello(dev=dev):
            pl.semaphore_signal(barrier, 1, device_id=dev, device_id_type=MESH)
        if cond is None:
            hello()
        else:
            pl.when(cond)(hello)
    pl.semaphore_wait(barrier, X + 1 + halves * (X - 1) + jnp.where(has_up, 1, 0) + jnp.where(has_dn, 1, 0))

    h_up = up_h.at[:, pl.ds(pl.multiple_of(y * half, half), half)]
    h_dn = dn_h.at[pl.ds(pl.multiple_of(y * half, half), half), :]
    o_up = up_h.at[:, pl.ds(pl.multiple_of((1 - y) * half, half), half)]
    o_dn = dn_h.at[pl.ds(pl.multiple_of((1 - y) * half, half), half), :]
    alls = (up_all, dn_all)

    def zsend(w, piece, src, way):
        dev, cond = ((to_zp, has_up), (to_zm, has_dn))[way]
        send(src, alls[w].at[piece], wsend.at[way, 0], wrecv.at[w, piece], dev, cond, track=False)

    late = z >= 2
    early = jnp.logical_not(late)
    for way in range(2):
        zsend(0, sp, h_up, way)
    zsend(1, sp, h_dn, 1)

    def own_dn():
        return rcopy(h_dn, dn_all.at[sp], wsend.at[0, 0], wrecv.at[1, sp], to_zp)

    @pl.when(late & has_up)
    def _():
        own_dn().start()

    for way, cond in enumerate((has_up, has_dn)):
        sent(up_all.at[pl.ds(0, 4)], wsend.at[way, 0], cond)
    hr = up_h.shape[0] // 2
    other = z * 2 + (1 - y)

    def ysend(w, src):
        send(src, alls[w].at[sp], wysend.at[w], wyrecv.at[w], to_y)

    def recv_y(w):
        recv(alls[w].at[other], wysend.at[w], wyrecv.at[w])

    def relays(w, k, yy):
        parts = []
        low, high = (z - k) * 2 + yy, (z + k) * 2 + yy
        for piece, way, cond in ((low, 0, (z >= k) & has_up), (high, 1, (z + k < Z) & has_dn)):
            ref, sem, dev = alls[w].at[piece], wsend.at[way, k], (to_zp, to_zm)[way]

            def go(ref=ref, sem=sem, dev=dev, piece=piece):
                recv(ref, sem, wrecv.at[w, piece])
                if halves and (w, k, yy) == (1, Z - 2, 1):
                    for h, (r0, nr, c0) in enumerate(pieces):
                        part = ref.at[pl.ds(r0, nr), pl.ds(c0, cw)]
                        rcopy(part, part, sem, wlast.at[h], dev).start()
                else:
                    rcopy(ref, ref, sem, wrecv.at[w, piece], dev).start()

            if (w, yy) == (1, 1):
                sent(up_all.at[pl.ds(0, 4)], sem, cond)
            parts.append((cond, go))
        return parts

    def fwd(w, k, yy):
        if k <= Z - 2:
            for cond, go in relays(w, k, yy):
                pl.when(cond)(go)

    def settle(w, piece):
        plane = piece // 2
        cond = ((plane < z) & jnp.logical_not(has_up)) | ((plane > z) & jnp.logical_not(has_dn))

        @pl.when(cond)
        def _():
            recv(alls[w].at[piece], wsend.at[0, 0], wrecv.at[w, piece])

    def angles(b):
        at = sp * nblk + b
        hc, hs = high[0, pl.ds(at, 1), :], high[1, pl.ds(at, 1), :]
        lc, ls = low[0], low[1]
        return hc * lc - hs * ls, hs * lc + hc * ls

    def rotated(blk, co, si):
        a, b = blk[:, : DK // 2].astype(F32), blk[:, DK // 2 :].astype(F32)
        return jnp.concatenate([a * co - b * si, a * si + b * co], axis=1)

    tot[...] = jnp.zeros_like(tot)
    for i in (2, 3, *range(10, len(loads)), 4, 5, 6):
        load(i).start()
    for i in (7, 8, 9, 0):
        load(i).wait()
    for h in range(heads):
        def state_block(t, after, h=h):
            b = nblk - 1 - t
            at = pl.ds(pl.multiple_of(b * BLOCK, BLOCK), BLOCK)
            row = ld[h : h + 1, pl.ds(pl.multiple_of(b * BLOCK, BLOCK), BLOCK)]
            i, j, cum_col, _, total = cumulative(row)
            co, si = angles(b)
            key = (rotated(k_v[at, h * DK : (h + 1) * DK], co, si) * DK ** (-0.5)).astype(BF16)
            kr[h, at, :] = key
            kd[at, :] = (key.astype(F32) * jnp.exp(total - cum_col + after)).astype(BF16)
            return after + total

        whole = lax.fori_loop(0, nblk, state_block, jnp.zeros((1, 1), F32))
        tot[h : h + 1, :] = jnp.broadcast_to(jnp.exp(whole), (1, tot.shape[1]))
        if h == 0:
            load(1).wait()
        s = lax.dot_general(kd[...], v_v[:, h * DV : (h + 1) * DV], (((0,), (0,)), ((), ())), preferred_element_type=F32)
        for p in range(2):
            part = s[:, p * DV // 2 : (p + 1) * DV // 2]
            stf[p, h] = part
            sth[p, h] = part.astype(BF16)
        send(sth.at[1 - y, h], yst.at[h], ssend.at[0], srecv.at[0], to_y, track=False)
    sent(sth.at[1 - y], ssend.at[0])
    send(tot, ytot, ssend.at[3], srecv.at[2], to_y)
    ysend(0, o_up)
    ysend(1, o_dn)

    load(2).wait()

    def local(h):
        strun[...] = jnp.zeros_like(strun)

        def span(t, before):
            at = pl.ds(pl.multiple_of(t * SPAN, SPAN), SPAN)
            row = ld[h : h + 1, pl.ds(pl.multiple_of(t * SPAN, SPAN), SPAN)]
            i, j, cum_col, cum_row, total = cumulative(row)
            parts = []
            for u in range(SPAN // BLOCK):
                co, si = angles(t * (SPAN // BLOCK) + u)
                qat = pl.ds(pl.multiple_of(t * SPAN + u * BLOCK, BLOCK), BLOCK)
                parts.append(rotated(q_v[qat, h * DK : (h + 1) * DK], co, si))
            query = jnp.concatenate(parts, axis=0).astype(BF16)
            key = kr[h, at, :]
            factor = jnp.where(i >= j, jnp.exp(jnp.minimum(cum_col - cum_row, 0.0)), 0.0)
            scores = lax.dot_general(query, key, (((1,), (1,)), ((), ())), preferred_element_type=F32)
            weights = (scores * factor).astype(BF16)
            q32 = query.astype(F32)
            val = v_v[at, h * DV : (h + 1) * DV]
            ret[at, h * DV : (h + 1) * DV] = dot(weights, val) + dot((q32 * jnp.exp(cum_col)).astype(BF16), strun[...].astype(BF16))
            q_v[at, h * DK : (h + 1) * DK] = (q32 * jnp.exp(cum_col + before)).astype(BF16)
            kdec = (key.astype(F32) * jnp.exp(total - cum_col)).astype(BF16)
            strun[...] = jnp.exp(total) * strun[...] + lax.dot_general(
                kdec, val, (((0,), (0,)), ((), ())), preferred_element_type=F32
            )
            return before + total

        lax.fori_loop(0, nspan, span, jnp.zeros((1, 1), F32))

    local(0)

    first = y == 0
    recv(ytot, ssend.at[3], srecv.at[2])
    recv(yst, ssend.at[0], srecv.at[0])

    def decays(h):
        own, oth = tot[h : h + 1, : DV // 2], ytot[h : h + 1, : DV // 2]
        return jnp.where(first, own, oth), jnp.where(first, oth, own)

    @pl.when(jnp.logical_not(has_dn))
    def _():
        crecv[...] = jnp.zeros_like(crecv)

    def s_pair(h):
        own, oth = stf[y, h], yst[h].astype(F32)
        return jnp.where(first, own, oth), jnp.where(first, oth, own)

    def chain(h):
        d0, d1 = decays(h)
        s0, s1 = s_pair(h)
        csend[h] = (d0 * d1 * crecv[h].astype(F32) + (d1 * s0 + s1)).astype(BF16)

    def chain_send(h):
        rcopy(csend.at[h], crecv.at[h], ssend.at[1], srecv.at[3 + h], to_zp).start()

    @pl.when(jnp.logical_not(has_dn))
    def _():
        for h in range(heads):
            chain(h)
            chain_send(h)
        own_dn().start()

    for h in range(1, heads):
        local(h)

    def part_up(part):
        ref = up_all.at[other, pl.ds(part * hr, hr)]
        rcopy(ref, ref, wsend.at[0, 0], wrecv.at[0, other], to_zp).start()

    @pl.when(late)
    def _():
        recv_y(0)
        pl.when(has_up)(lambda: part_up(0))

    @pl.when(has_dn)
    def _():
        for h in range(heads):
            recv(crecv.at[h], ssend.at[1], srecv.at[3 + h])

            @pl.when(has_up)
            def _():
                chain(h)
                chain_send(h)

        @pl.when(early & has_up)
        def _():
            own_dn().start()

    def chain_end():
        rcopy(csend, crecv, ssend.at[1], srecv.at[0], to_zp).wait_send()

    pending.append((has_up, chain_end))
    for h in range(heads):
        d0, _ = decays(h)
        s0, _ = s_pair(h)
        got = crecv[h].astype(F32)
        later = (d0 * got + s0).astype(BF16)
        inc[y, h] = jnp.where(first, crecv[h], later)
        esend[h] = jnp.where(first, later, crecv[h])
        send(esend.at[h], inc.at[y, h], ssend.at[2], srecv.at[1], to_y, track=False)
    @pl.when(early)
    def _():
        recv_y(0)
        pl.when(has_up)(lambda: part_up(0))

    pl.when(has_up)(lambda: part_up(1))
    zsend(0, other, up_all.at[other], 1)
    fwd(0, 1, y)
    load(3).wait()
    for i in range(stack):
        load(10 + i).wait()
    sent(esend, ssend.at[2])
    recv(inc.at[1 - y], ssend.at[2], srecv.at[1])

    ph = mine // 2
    fr = min(128, ph)

    def finish(base):

        def part(t, carry):
            at = pl.ds(pl.multiple_of(base + t * fr, fr), fr)
            for h in range(heads):
                qd = q_v[at, h * DK : (h + 1) * DK]
                r = ret[at, h * DV : (h + 1) * DV] + jnp.concatenate([dot(qd, inc[0, h]), dot(qd, inc[1, h])], axis=1)
                normed = r * lax.rsqrt(jnp.mean(r * r, axis=1, keepdims=True) + EPS)
                g = g_v[at, h * DV : (h + 1) * DV].astype(F32)
                g_v[at, h * DV : (h + 1) * DV] = (g / (1.0 + jnp.exp(-g)) * normed).astype(BF16)
            return carry

        lax.fori_loop(0, ph // fr, part, 0)

    pt = min(512, wc)

    def project(base, put):
        rows_at = pl.ds(pl.multiple_of(base, ph), ph)
        for i in range(stack):
            def part(t, carry, i=i):
                at = pl.ds(pl.multiple_of(t * pt, pt), pt)
                to = pl.ds(pl.multiple_of(i * wc + t * pt, pt), pt)
                put(to, dot(g_v[rows_at, :], wide[i * hv : (i + 1) * hv, at]))
                return carry

            lax.fori_loop(0, wc // pt, part, 0)

    def for_sibling(j, p):
        base = (xat(j) * 2 + (1 - c)) * mine + p * ph
        finish(base)
        mid = pl.ds(p * ph, ph)

        def put(at, val):
            pp[j, mid, at] = val.astype(BF16)

        project(base, put)
        send(pp.at[j, mid], pr.at[j, mid], psend.at[j], precv.at[j, p], to_c, track=False)

    def for_mine(j, p):
        base = (xat(j) * 2 + c) * mine + p * ph
        finish(base)
        mid = pl.ds(p * ph, ph)

        def put(at, val):
            acc[mid, at] = val.astype(BF16).astype(F32)

        project(base, put)
        recv(pr.at[j, mid], psend.at[j], precv.at[j, p])
        if j:
            for r in range(p * ROWS // 2, (p + 1) * ROWS // 2):
                at = pl.ds(r * rc, rc)
                psum[j - 1, at, :] = (acc[at, :] + pr[j, at, :].astype(F32)).astype(BF16)
                send(psum.at[j - 1, at], xr.at[j - 1, at], xsend.at[j - 1], xrecv.at[j - 1, r], to_x(j), track=False)

    for j in range(1, X):
        for p in range(2):
            for_sibling(j, p)
            for_mine(j, p)
    fwd(0, 1, 1 - y)
    for p in range(2):
        for_sibling(0, p)
        for_mine(0, p)
    recv_y(1)
    for way in range(2):
        zsend(1, other, dn_all.at[other], way)
    fwd(0, 2, y)

    for j in range(X):
        sent(pp.at[j], psend.at[j])
        if j:
            sent(psum.at[j - 1], xsend.at[j - 1])

    load(4).wait()
    for r in range(ROWS):
        at = pl.ds(r * rc, rc)
        s = acc[at, :] + pr[0, at, :].astype(F32)
        for j in range(1, X):
            recv(xr.at[j - 1, at], xsend.at[j - 1], xrecv.at[j - 1, r])
            s = s + xr[j - 1, at, :].astype(F32)
        u = (res_v[at, :].astype(F32) + s).astype(BF16)
        upd[at, :] = u
        u = u.astype(F32)
        u = u * lax.rsqrt(jnp.mean(u * u, axis=1, keepdims=True) + EPS)
        x_all[c, y, x, at, :] = (u * gain[...].astype(F32).reshape(1, d)).astype(BF16)
        own = x_all.at[c, y, x, at]
        send(own, own, asend.at[0, 0], ary.at[0, r], to_y, track=False)
        for j in range(1, X):
            send(own, own, asend.at[1, j], arx.at[j - 1, r], to_x(j), track=False)
        send(own, own, asend.at[2, 0], ard.at[0, 0], to_c, track=False)

    load(5).wait()
    for k in range(1, Z - 1):
        if k == 1:
            continue
        fwd(0, k, 1 - y)
        if k > 2:
            fwd(0, k, y)

    ht = min(512, half)

    def hid_rows(yy, xx):
        return pl.ds(pl.multiple_of((yy * X + xx) * mine, mine), mine)

    def hid_of(cc):
        return pl.ds(pl.multiple_of(cc * half, half), half)

    def hidden(yy, xx):
        def part(t, carry):
            at = pl.ds(pl.multiple_of(t * ht, ht), ht)
            w = up_all[:, :, at].reshape(d, ht)
            for cc in range(2):
                pre = jnp.maximum(dot(x_all[cc, yy, xx], w), 0.0)
                col = pl.ds(pl.multiple_of(cc * half + t * ht, ht), ht)
                wide[hid_rows(yy, xx), col] = (pre * pre).astype(BF16)
            return carry

        lax.fori_loop(0, half // ht, part, 0)

    for i in range(X):
        for kind, yy in ((0, y), (2, y), (3, 1 - y)):
            sent(x_all.at[c, yy, xat(-i)], asend.at[kind, i])
        if i:
            sent(x_all.at[c, y, x], asend.at[1, i])

    def from_sibling(yrel, i):
        recv(x_all.at[1 - c, (1 - y) if yrel else y, xat(-i)], asend.at[2, 0], ard.at[yrel, i])

    def pass_on(yrel, i, r):
        at = pl.ds(r * rc, rc)
        ref = x_all.at[c, (1 - y) if yrel else y, xat(-i), at]
        if yrel:
            recv(ref, asend.at[0, 0], ary.at[i, r])
        else:
            recv(ref, asend.at[1, i], arx.at[i - 1, r])
            send(ref, ref, asend.at[0, i], ary.at[i, r], to_y, track=False)
        send(ref, ref, asend.at[2 + yrel, i], ard.at[yrel, i], to_c, track=False)

    for r in range(ROWS):
        pass_on(1, 0, r)
    for r in range(ROWS):
        for j in range(1, X):
            pass_on(0, j, r)
        if r == 1:
            fwd(1, 1, 0)
    fwd(1, 1, 1)
    for k in range(n_sp):
        settle(0, k)
    from_sibling(0, 0)
    hidden(y, x)
    from_sibling(1, 0)
    hidden(1 - y, x)
    for j in range(1, X):
        for r in range(ROWS):
            pass_on(1, j, r)
        from_sibling(0, j)
        hidden(y, xat(-j))
    for j in range(1, X):
        from_sibling(1, j)
        hidden(1 - y, xat(-j))

    load(6).wait()
    m = jnp.minimum(z, Z - 1 - z)
    hm = mine // 2

    def block_of(s):
        i = s // 2
        near = jnp.where(i % 2 == 1, z - (i + 1) // 2, z + i // 2)
        far = jnp.where(z <= Z - 1 - z, i, Z - 1 - i)
        return jnp.where(i <= 2 * m, near, far) * 2 + s % 2

    units = n_sp - 1 if halves else n_sp
    total = units + 2 if halves else units
    na, nb = 3 * X - 2, X

    class Unit:
        def __init__(self, t, part=None):
            self.t, self.u, self.part = t, (t if part is None else n_sp - 1), part
            self.w = cols if part is None else cw
            self.c0 = 0 if part is None else part * cw
            self.block = block_of(self.u)

        def trim(self, ref, start):
            return ref if self.w == cols else ref.at[..., pl.ds(start, self.w)]

        def bulk(self, n, ss, rs):
            ref = wide.at[pl.ds(0, n * hm), pl.ds(0, self.w)]
            return rcopy(ref, ref, ss, rs, to_c)

        def to_sib(self):
            t = self.t
            return rcopy(self.trim(pd.at[t % 2], 0), self.trim(r1.at[self.u], self.c0), dsem.at[t % 2], drecv.at[t], to_c)

        def copies(self, stage):
            q, t, u = qs.at[self.t % SLOTS], self.t, self.u
            if stage == 0:
                pairs = [(q.at[1 - y, :, 0], r2y.at[u], to_y)]
                pairs += [(q.at[:, xat(j), 1], r2x.at[u, j - 1], to_x(j)) for j in range(1, X)]
            else:
                pairs = [(q.at[1 - y, x, 1], r3y.at[u], to_y)]
                pairs += [(q.at[y, xat(j), 0], r3x.at[u, j - 1], to_x(j)) for j in range(1, X)]
            if self.part is not None:
                to = [(1, 0, to_y)] + [(0, j, to_x(j)) for j in range(1, X)] + [(1, j, to_diag(j)) for j in range(1, X)]
                pairs = [(q.at[(1 - y) if f else y, xat(j)], rd.at[self.part, f * X + j], dev) for f, j, dev in to]
            for src, dst, dev in pairs:
                dst = dst if self.part is not None else self.trim(dst, self.c0)
                rcopy(self.trim(src, 0), dst, qsem.at[stage, t % SLOTS], qrecv.at[stage, t], dev).start()

        def wait_sib(self):
            ref = self.trim(pd.at[self.t % 2], 0)
            rcopy(ref, ref, dsem.at[self.t % 2], drecv.at[self.t], to_c).wait_send()

        def arrive(self, i):
            r0, nr, c0 = pieces[i]

            @pl.when(jnp.logical_not(has_up & has_dn))
            def _():
                ref = dn_all.at[self.block, pl.ds(r0, nr), pl.ds(c0, cw)]
                recv(ref, wsend.at[0, 0], wlast.at[i])

        def product(self, cls, r0, nr):
            w = dn_all[self.block, r0 : r0 + nr, self.c0 : self.c0 + self.w]
            return dot(wide[:, pl.ds(pl.multiple_of(cls * half + r0, 128), nr)], w)

        def compute(self, before):
            if self.part is None:
                settle(1, self.block)
            else:
                self.arrive(0)
            before()
            self.offer(self.product(1 - c, 0, half))
            ret[: 2 * X * mine, : self.w] = self.product(c, 0, half)

        def offer(self, value):
            pd[self.t % 2, :, :, :, :, : self.w] = value.astype(BF16).reshape(2, X, 2, hm, self.w)
            self.to_sib().start()

        def compute_late(self, before):
            near = slice(cw, 2 * cw), slice(2 * cw, 3 * cw)
            self.arrive(1)
            ret[: 2 * X * mine, near[0]] = self.product(1 - c, 0, ka)
            ret[: 2 * X * mine, near[1]] = self.product(c, 0, ka)
            before()
            self.arrive(2)
            self.offer(ret[: 2 * X * mine, near[0]] + self.product(1 - c, ka, half - ka))
            ret[: 2 * X * mine, :cw] = ret[: 2 * X * mine, near[1]] + self.product(c, ka, half - ka)

        def first(self):
            k, at = self.t % SLOTS, slice(self.c0, self.c0 + self.w)
            self.to_sib().wait_recv()
            own = ret[: 2 * X * mine, : self.w].reshape(2, X, 2, hm, self.w)
            qs[k, :, :, :, :, : self.w] = (own.astype(BF16).astype(F32) + r1[self.u, :, :, :, :, at].astype(F32)).astype(BF16)
            self.copies(0)

        def second(self):
            k, at, w = self.t % SLOTS, slice(self.c0, self.c0 + self.w), self.w
            self.bulk(na, qsem.at[0, 0], qrecv.at[0, self.t]).wait_recv()
            qs[k, y, :, 0, :, :w] = (qs[k, y, :, 0, :, :w].astype(F32) + r2y[self.u, :, :, at].astype(F32)).astype(BF16)
            s = qs[k, :, x, 1, :, :w].astype(F32)
            for j in range(1, X):
                s = s + r2x[self.u, j - 1, :, :, at].astype(F32)
            qs[k, :, x, 1, :, :w] = s.astype(BF16)
            self.copies(1)

        def final(self):
            k, at, w = self.t % SLOTS, slice(self.c0, self.c0 + self.w), self.w
            col = pl.ds(pl.multiple_of(self.block * cols + self.c0, 128), w)
            if self.part is not None:
                every = (2 * X - 1) * 2
                self.bulk(every, qsem.at[0, 0], qrecv.at[0, self.t]).wait_recv()
                s = qs[k, y, x, :, :, :w].astype(F32)
                for i in range(1, 2 * X):
                    s = s + rd[self.part, i].astype(F32)
                out[:, col] = (upd[:, col].astype(F32) + s.reshape(mine, w)).astype(BF16)
                self.bulk(every, qsem.at[0, k], qrecv.at[0, 0]).wait_send()
                return
            self.bulk(nb, qsem.at[1, 0], qrecv.at[1, self.t]).wait_recv()
            s = upd[:hm, col].astype(F32) + qs[k, y, x, 0, :, :w].astype(F32)
            for j in range(1, X):
                s = s + r3x[self.u, j - 1, :, at].astype(F32)
            out[:hm, col] = s.astype(BF16)
            s = upd[hm:, col].astype(F32) + qs[k, y, x, 1, :, :w].astype(F32) + r3y[self.u, :, at].astype(F32)
            out[hm:, col] = s.astype(BF16)
            self.bulk(na, qsem.at[0, k], qrecv.at[0, 0]).wait_send()
            self.bulk(nb, qsem.at[1, k], qrecv.at[1, 0]).wait_send()

    last = [(2 * (k - 2 + yy), relays(1, k, yy)) for k in range(2, Z - 1) for yy in range(2)]

    def step(s, carry):
        for at, parts in last:
            for cond, go in parts:
                pl.when(cond & (s == at))(go)
        Unit(s).compute(lambda: pl.when(s >= 2)(lambda: Unit(s - 2).wait_sib()))

        @pl.when(s >= 2)
        def _():
            Unit(s - 2).second()

        Unit(s).first()

        @pl.when(s >= 4)
        def _():
            Unit(s - 4).final()

        return carry

    lax.fori_loop(0, units, step, 0)
    tail = [Unit(t) for t in range(units)]

    def finish_unit(t):
        tail[t].final()

    if halves:
        tail += [Unit(units + p, p) for p in range(2)]
        one, two = tail[units], tail[units + 1]
        one.compute(tail[units - 2].wait_sib)
        tail[units - 2].second()
        one.first()
        finish_unit(units - 4)
        two.compute_late(tail[units - 1].wait_sib)
        tail[units - 1].second()
        two.first()
        finish_unit(units - 3)
    else:
        tail[units - 2].second()
        tail[units - 1].second()
    for t in range(total - 4, total):
        finish_unit(t)
    for t in range(total - 2, total):
        tail[t].wait_sib()
    for cond, end in pending:
        if cond is None:
            end()
        else:
            pl.when(cond)(end)


def body(n_sp, n_tp, resid, queries, keys, values, gates, log_decay, w_out, gain, up, down):
    X, Z = n_tp // 2, n_sp // 2
    rows, heads = queries.shape[0], log_decay.shape[0]
    mine, d = resid.shape
    half, cols, part = up.shape[1] // 2, down.shape[1], up.shape[0]
    freq = 10000.0 ** (-np.arange(0, DK, 2, dtype=np.float64) / DK)
    near = np.arange(BLOCK)[:, None] * freq[None, :]
    far = (BLOCK * np.arange(rows * n_sp // BLOCK))[:, None] * freq[None, :]
    tables = [jnp.asarray(np.stack([np.cos(a), np.sin(a)]), F32) for a in (near, far)]
    vm, anym = pl.BlockSpec(memory_space=pltpu.VMEM), pl.BlockSpec(memory_space=pl.ANY)
    dma = pltpu.SemaphoreType.DMA
    V = pltpu.VMEM
    hd, hv = heads * DK, heads * DV
    sq = (DK, DV // 2)
    scratch = [
        V((heads, rows), F32), *[V(t.shape, F32) for t in tables],
        V((rows, hd), BF16), V((rows, hd), BF16), V((rows, hv), BF16), V((rows, hv), BF16),
        V((2 * X * mine, 2 * half), BF16), V((mine, d), BF16),
        V((heads, rows, DK), BF16), V((rows, DK), BF16),
        V((2, heads, *sq), F32), V((2, heads, *sq), BF16), V((DK, DV), F32),
        V((heads, *sq), BF16), V((8, DV // 2), F32), V((8, DV // 2), F32),
        V((heads, *sq), BF16), V((heads, *sq), BF16), V((heads, *sq), BF16), V((2, heads, *sq), BF16),
        V((rows, hv), F32),
        V((X, mine, d), BF16), V((X, mine, d), BF16), V((X - 1, mine, d), BF16), V((X - 1, mine, d), BF16),
        V((mine, d), F32), V((mine, d), BF16),
        V((2, 2, X, mine, d), BF16), V((n_sp, part, half), BF16), V((n_sp, half, cols), BF16),
        V((2, 2, X, 2, mine // 2, cols), BF16),
        V((SLOTS, 2, X, 2, mine // 2, cols), BF16), V((n_sp, 2, X, 2, mine // 2, cols), BF16),
        V((n_sp, X, mine // 2, cols), BF16), V((n_sp, X - 1, 2, mine // 2, cols), BF16),
        V((n_sp, mine // 2, cols), BF16), V((n_sp, X - 1, mine // 2, cols), BF16),
        V((2, 2 * X, 2, mine // 2, cols // 2), BF16),
        dma((10 + 2 * X * mine // hv,)), dma((2, max(1, n_sp // 2 - 1))), dma((2, n_sp)), dma((3,)), dma((2,)), dma((2,)),
        dma((4,)), dma((3 + heads,)), dma((X,)), dma((X, 2)), dma((X - 1,)), dma((X - 1, ROWS)),
        dma((4, X)), dma((X - 1, ROWS)), dma((X, ROWS)), dma((2, X)),
        dma((2,)), dma((n_sp + 1,)), dma((2, SLOTS)), dma((2, n_sp + 1)),
    ]
    return pl.pallas_call(
        functools.partial(kernel, n_sp, n_tp),
        in_specs=[anym] * 7 + [vm] + [anym] * 4,
        out_specs=vm,
        out_shape=pltpu.VMEM((mine, d), BF16),
        scratch_shapes=scratch,
        compiler_params=pltpu.CompilerParams(
            collective_id=0, has_side_effects=True, vmem_limit_bytes=62 * 2**20
        ),
        name="layer",
    )(resid, queries, keys, values, gates, log_decay, w_out, gain, up, down, *tables)


def solution(mesh):
    placed = (
        P(("sp", "tp"), None),
        P("sp", "tp"),
        P("sp", "tp"),
        P("sp", "tp"),
        P("sp", "tp"),
        P("tp", "sp"),
        P("tp", None),
        P(),
        P("sp", "tp"),
        P("tp", "sp"),
    )
    return jax.shard_map(
        functools.partial(body, mesh.shape["sp"], mesh.shape["tp"]),
        mesh=mesh,
        in_specs=placed,
        out_specs=P(("sp", "tp"), None),
        check_vma=False,
    )
```
